32 devices in a mesh: st: 8 (over z, x), tp: 4 (over y, core).
Axes of the slice: x: 2, y: 2, z: 4, core: 2. Of those that a mesh axis runs over, the one named last changes fastest.
Arguments:
- tokens: bfloat16 [16384, 2048], P('st', 'tp'), may hold values from -48 to 48
- store: bfloat16 [256, 64, 2048], P('st'), may hold values from -48 to 48
- passage_holder_index: int32 [128, 2], P('st'), may hold values from 0 to 7, all different within a row; in each aligned block of 16 rows (0 to 15, 16 to 31, ...) at most 8 rows name the same one
- passage_slot: int32 [128, 2], P('st'), may hold values from 0 to 31
- query_weight: bfloat16 [2048, 1024], P(None, 'tp'), may hold values from -0.125 to 0.125
- key_matrix: bfloat16 [2048, 1024], P(None, 'tp'), may hold values from -0.125 to 0.125
- value_weight: bfloat16 [2048, 1024], P(None, 'tp'), may hold values from -0.125 to 0.125
- outer_gate: bfloat16 [2048, 1024], P(None, 'tp'), may hold values from -0.125 to 0.125
- inner_gate: bfloat16 [2048, 1024], P(None, 'tp'), may hold values from -0.125 to 0.125
- conv_input: bfloat16 [2048, 1024], P(None, 'tp'), may hold values from -0.125 to 0.125
- conv_taps: bfloat16 [3, 1024], P(None, 'tp'), may hold values from -3.5 to 3.5
- route_gate_projection: bfloat16 [2048, 2], replicated, may hold values from -0.125 to 0.125
- conv_out: bfloat16 [1024, 2048], P('tp'), may hold values from -0.1875 to 0.1875
- memory_out: bfloat16 [1024, 2048], P('tp'), may hold values from -0.1875 to 0.1875
Outputs:
- mixed: bfloat16 [16384, 2048], P(('st', 'tp'))
The draws below stay inside these ranges and needn't reach their ends.
Inputs may be any that keep to these rules, and one draw needn't show every extreme that they name: `passage_holder_index`: each row names 2 different owners; among the rows of one index of st (16 aligned rows) no owner is named more than 8 times, a bound that some index of st reaches.
All inputs are finite; a program needn't handle non-finite values.
Results may differ from the reference program's by a relative error of at most 0.014.
Values may be sent and summed in bfloat16 or wider, within the bound.
A program may use at most 128 MiB of HBM per device.

```python
import math
import jax
import jax.numpy as jnp
import numpy as np
from jax import lax

D = 2048
HEADS = 8
HEAD_SIZE = 128
FILTER_CHANNELS = 1024
CONV_K = 3
SEQ_LEN = 256
BLOCK = 128
NPB = 2
PLEN = 64
P_DEV = 32
MEM_WIDTH = 1024
NBLK_DEV = 16
CAP = 8
TOKENS = 16384
BLOCKS = 128
PASSAGES = 256
N_ST = 8
N_TP = 4


def draw_tokens(key, part):
    first_key = jax.random.fold_in(jax.random.fold_in(key, 11), 0)
    values = jnp.clip(jax.random.normal(first_key, (TOKENS, D), jnp.float32), -4.0, 4.0)
    return values.astype(jnp.bfloat16)


def draw_store(key, part):
    first_key = jax.random.fold_in(jax.random.fold_in(key, 23), 0)
    values = jnp.clip(jax.random.normal(first_key, (PASSAGES, PLEN, D), jnp.float32), -4.0, 4.0)
    return values.astype(jnp.bfloat16)


def set_ends(values, key, smallest, high):
    shape = values.shape
    spot = [jax.random.randint(jax.random.fold_in(key, axis), (), 0, shape[axis]) for axis in range(len(shape))]
    values = values.at[tuple(spot)].set(smallest)
    longest = shape.index(max(shape))
    spot[longest] = (spot[longest] + 1) % shape[longest]
    return values.at[tuple(spot)].set(high)


def shard_levels(key, dims, pieces, low, largest):
    level = 1.0
    for dim, shards_of in pieces:
        draws = jax.random.uniform(jax.random.fold_in(jax.random.fold_in(key, 6), dim), (shards_of,), jnp.float32, low / len(pieces), largest / len(pieces))
        level = level * jnp.repeat(jnp.exp(draws), dims[dim] // shards_of).reshape((-1,) + (1,) * (len(dims) - 1 - dim))
    return level


def rank_bounds(count, skew):
    weights = [(1 << 20) // math.isqrt(standing ** skew) + 1 for standing in range(1, count + 1)]
    scale = 1 + sum(weights) // (1 << 30)
    return np.cumsum(np.array([max(1, weight // scale) for weight in weights]))


def skewed_ids(own_key, extent, amount, skew):
    listing = rank_bounds(amount, skew)
    pick = jax.random.randint(jax.random.fold_in(own_key, 1), extent, 0, int(listing[amount - 1]))
    standing = jnp.searchsorted(jnp.asarray(listing, jnp.int32), pick, side="right")
    return jax.random.permutation(jax.random.fold_in(own_key, 2), amount)[standing].astype(jnp.int32)


def assign_block(rng, own, number, rows, count, top, limit, lean):
    sequence = jax.random.permutation(rng, count)
    heavy_load, ordinary = shares(count, rows * top, limit, lean, True), shares(count, rows * top, limit, lean, False)
    places = jnp.arange(count)

    def named(tallies, rotation):
        used = int((tallies > 0).sum())
        fixed = max(1, used // 4)
        moved = fixed + (places - fixed + rotation * (used - fixed)) % max(1, count - fixed)
        return jnp.zeros((count,), jnp.int32).at[sequence[jnp.where(places < fixed, places, moved)]].set(jnp.asarray(tallies, jnp.int32))

    tallies = jnp.where(number % 4 == 0, named(heavy_load, number // 4), named(ordinary, number - number // 4 - 1))
    mixed = jax.random.permutation(jax.random.fold_in(own, 3), count)
    donor, sink = mixed[0:count // 2 * 2:2], mixed[1:count // 2 * 2:2]
    slack = jnp.minimum(tallies[donor] - 1, limit - tallies[sink]) // 2
    slack = jnp.where((donor == sequence[0]) | (sink == sequence[0]) | (tallies[sink] == 0), 0, jnp.maximum(slack, 0))
    moved = jax.random.randint(jax.random.fold_in(own, 4), (count // 2,), 0, 1 << 20) % (slack + 1)
    tallies = tallies.at[donor].add(-moved).at[sink].add(moved)
    members = jnp.searchsorted(jnp.cumsum(tallies), jnp.arange(rows * top), side="right").astype(jnp.int32)
    listing = members.reshape(top, rows).T
    listing = listing[jax.random.permutation(jax.random.fold_in(own, 1), rows)]
    rotation = jax.random.randint(jax.random.fold_in(own, 2), (rows, 1), 0, top)
    return jnp.take_along_axis(listing, (jnp.arange(top)[None, :] + rotation) % top, axis=1)


def shares(count, total, limit, slope, full):
    loads = [(1 << 20) // math.isqrt(grade ** slope) + 1 for grade in range(1, count + 1)]
    largest = limit if full else min(limit, max(-(-total // count), total * loads[0] // sum(loads)))
    least = 1 if total - largest >= count - 1 else 0
    counts, rest = [largest] + [least] * (count - 1), total - largest - least * (count - 1)
    while rest > 0:
        candidates = [i for i in range(1, count) if counts[i] < largest] or [i for i in range(1, count) if counts[i] < limit]
        pool, budget = sum([loads[i] for i in candidates]), rest
        for i in candidates:
            more = min(limit - counts[i], max(1, budget * loads[i] // pool), rest)
            counts[i] = counts[i] + more
            rest = rest - more
    return np.array(counts)


def bell_draw(rng, dims, deviation, bound, cuts=(), held_as=jnp.bfloat16):
    entries = jax.random.normal(rng, dims, jnp.float32) * deviation
    if len(cuts) > 0:
        entries = shard_levels(rng, dims, cuts, -0.22, 0.18) * entries
    return jnp.clip(entries, min=-bound, max=bound).astype(held_as)


def setup_inputs(seed: int = 0) -> dict:
    splits = jax.random.split(jax.random.key(seed), 15)
    tokens = draw_tokens(jax.random.fold_in(splits[14], 71), 0)
    store = draw_store(jax.random.fold_in(splits[14], 71), 0)
    passage_holder_index_keys = jax.random.split(jax.random.fold_in(splits[2], 1), BLOCKS // NBLK_DEV)
    passage_holder_index_turns = jax.random.permutation(jax.random.fold_in(splits[2], 3), BLOCKS // NBLK_DEV)
    passage_holder_index = jax.vmap(lambda own, number: assign_block(jax.random.fold_in(splits[2], 2), own, number, NBLK_DEV, N_ST, NPB, CAP, 2))(passage_holder_index_keys, passage_holder_index_turns).reshape((BLOCKS, NPB))
    passage_slot = set_ends(skewed_ids(splits[3], (BLOCKS, NPB), P_DEV, 2), jax.random.fold_in(splits[3], 3), 0, P_DEV - 1).astype(jnp.int32)
    query_weight = bell_draw(splits[4], (D, MEM_WIDTH), D ** -0.5, 0.125, ((1, 4),))
    key_matrix = bell_draw(splits[5], (D, MEM_WIDTH), D ** -0.5, 0.125, ((1, 4),))
    value_weight = bell_draw(splits[6], (D, MEM_WIDTH), D ** -0.5, 0.125, ((1, 4),))
    outer_gate = bell_draw(splits[7], (D, FILTER_CHANNELS), D ** -0.5, 0.125, ((1, 4),))
    inner_gate = bell_draw(splits[8], (D, FILTER_CHANNELS), D ** -0.5, 0.125, ((1, 4),))
    conv_input = bell_draw(splits[9], (D, FILTER_CHANNELS), D ** -0.5, 0.125, ((1, 4),))
    conv_taps = bell_draw(splits[10], (CONV_K, FILTER_CHANNELS), CONV_K ** -0.5, 3.5, ((1, 4),))
    route_gate_projection = bell_draw(splits[11], (D, 2), D ** -0.5, 0.125)
    conv_out = bell_draw(splits[12], (FILTER_CHANNELS, D), FILTER_CHANNELS ** -0.5, 0.1875, ((0, 4),))
    memory_out = bell_draw(splits[13], (MEM_WIDTH, D), MEM_WIDTH ** -0.5, 0.1875, ((0, 4),))
    return {"tokens": tokens, "store": store, "passage_holder_index": passage_holder_index, "passage_slot": passage_slot, "query_weight": query_weight, "key_matrix": key_matrix, "value_weight": value_weight, "outer_gate": outer_gate, "inner_gate": inner_gate, "conv_input": conv_input, "conv_taps": conv_taps, "route_gate_projection": route_gate_projection, "conv_out": conv_out, "memory_out": memory_out}


def reference(tokens, store, passage_holder_index, passage_slot, query_weight, key_matrix, value_weight, outer_gate, inner_gate, conv_input, conv_taps, route_gate_projection, conv_out, memory_out):
    queries = jnp.dot(tokens, query_weight, preferred_element_type=jnp.float32).astype(jnp.bfloat16)
    outer_part = jnp.dot(tokens, outer_gate, preferred_element_type=jnp.float32)
    inner_part = jnp.dot(tokens, inner_gate, preferred_element_type=jnp.float32)
    value_part = jnp.dot(tokens, conv_input, preferred_element_type=jnp.float32)
    branch_mix = jax.nn.sigmoid(jnp.dot(tokens, route_gate_projection, preferred_element_type=jnp.float32))
    mixed_input = (inner_part * value_part).reshape(TOKENS // SEQ_LEN, SEQ_LEN, FILTER_CHANNELS)
    padded_input = jnp.pad(mixed_input, ((0, 0), (CONV_K - 1, 0), (0, 0)))
    tap_values = conv_taps.astype(jnp.float32)
    filtered_signal = tap_values[0] * padded_input[:, 0:SEQ_LEN]
    for offset in range(1, CONV_K):
        filtered_signal = filtered_signal + tap_values[offset] * padded_input[:, offset:offset + SEQ_LEN]
    conv_branch = (outer_part * filtered_signal.reshape(TOKENS, FILTER_CHANNELS)).astype(jnp.bfloat16)

    passage_ids = (passage_holder_index * P_DEV + passage_slot).reshape(-1).astype(jnp.int32)
    memory_rows = store[passage_ids].reshape(-1, D)
    passage_key_rows = jnp.dot(memory_rows, key_matrix, preferred_element_type=jnp.float32).astype(jnp.bfloat16)
    retrieved_content_vectors = jnp.dot(memory_rows, value_weight, preferred_element_type=jnp.float32).astype(jnp.bfloat16)
    passage_key_rows = passage_key_rows.reshape(BLOCKS, NPB * PLEN, HEADS, HEAD_SIZE)
    retrieved_content_vectors = retrieved_content_vectors.reshape(BLOCKS, NPB * PLEN, HEADS, HEAD_SIZE)
    query_block_rows = queries.reshape(BLOCKS, BLOCK, HEADS, HEAD_SIZE)
    scores = jnp.einsum('bqhd,bkhd->bhqk', query_block_rows.astype(jnp.float32), passage_key_rows.astype(jnp.float32)) * (HEAD_SIZE ** -0.5)
    softmax_shares = jax.nn.softmax(scores, axis=-1).astype(jnp.bfloat16)
    memory_branch = jnp.einsum('bhqk,bkhd->bqhd', softmax_shares.astype(jnp.float32), retrieved_content_vectors.astype(jnp.float32))
    memory_branch = memory_branch.reshape(TOKENS, MEM_WIDTH).astype(jnp.bfloat16)

    conv_cols = FILTER_CHANNELS // N_TP
    head_cols = MEM_WIDTH // N_TP
    summed = jnp.zeros((TOKENS, D), jnp.float32)
    for tensor_parallel_team in range(N_TP):
        conv_slice = conv_branch[:, tensor_parallel_team * conv_cols:(tensor_parallel_team + 1) * conv_cols]
        memory_slice = memory_branch[:, tensor_parallel_team * head_cols:(tensor_parallel_team + 1) * head_cols]
        share_term = (branch_mix[:, 0:1] * jnp.dot(conv_slice, conv_out[tensor_parallel_team * conv_cols:(tensor_parallel_team + 1) * conv_cols], preferred_element_type=jnp.float32)
                      + branch_mix[:, 1:2] * jnp.dot(memory_slice, memory_out[tensor_parallel_team * head_cols:(tensor_parallel_team + 1) * head_cols], preferred_element_type=jnp.float32))
        summed = summed + lax.optimization_barrier(share_term.astype(jnp.bfloat16)).astype(jnp.float32)
    return summed.astype(jnp.bfloat16)
```

```python
import functools

import jax
import jax.numpy as jnp
from jax import lax
from jax.experimental import pallas as pl
from jax.experimental.pallas import tpu as pltpu
from jax.sharding import PartitionSpec as P

HEAD_SIZE = 128
CONV_K = 3
SEQ_LEN = 256
BLOCK = 128
NPB = 2
PLEN = 64
CORES = 2
LANES = 128
MESH = pl.DeviceIdType.MESH


def flip(index, mask):
    result, bit = index, 1
    while bit <= mask:
        if mask & bit:
            result = result + bit * (1 - 2 * ((index // bit) % 2))
        bit *= 2
    return result


def aligned(start, size):
    return pl.ds(pl.multiple_of(start * size, size), size)


def fused_kernel(
    sizes,
    target_ref,
    mine_ref,
    ask_ref,
    tokens_ref,
    store_ref,
    key_ref,
    value_ref,
    query_ref,
    outer_ref,
    inner_ref,
    conv_ref,
    taps_ref,
    gate_ref,
    conv_out_ref,
    memory_out_ref,
    out_ref,
    tok,
    passages,
    in_weight,
    kv_weight,
    out_weight,
    total,
    queries,
    gates,
    result,
    wanted,
    wanted_smem,
    *rest,
):
    owners, team, heads, capacity, rows, feat = sizes
    chips = team // CORES
    own_rows = rows // team
    chunks = rows // SEQ_LEN
    refs = iter(rest)
    table = [next(refs) for _ in range(heads)]
    staged = [next(refs) for _ in range(heads)]
    served = [next(refs) for _ in range(heads)]
    branch = [next(refs) for _ in range(2 * heads)]
    moved = [next(refs) for _ in range(2 * heads)]
    (
        load_sem,
        store_sem,
        smem_sem,
        ask_send,
        ask_recv,
        near_send,
        near_recv,
        far_send,
        far_recv,
        pass_send,
        pass_recv,
        serve_send,
        serve_recv,
        row_send,
        row_recv,
        w_near_send,
        w_near_recv,
        w_far_send,
        w_far_recv,
        w_side_send,
        w_side_recv,
        w_pass_send,
        w_pass_recv,
        out_sem,
    ) = refs

    st = lax.axis_index("st")
    me = lax.axis_index("tp")
    chip, core = me // CORES, me % CORES
    partner = chip * CORES + 1 - core
    side = flip(st, 1)
    half = st % 2

    def up(k):
        return lax.rem(chip + k, chips) * CORES + core

    def down(k):
        return lax.rem(chip + chips - k, chips) * CORES + core

    def down_other(k):
        return lax.rem(chip + chips - k, chips) * CORES + 1 - core

    passage_rows = passages.shape[0]
    pieces = 4
    piece = passage_rows // pieces
    loads = []
    for h in range(heads):
        lanes = slice(h * HEAD_SIZE, (h + 1) * HEAD_SIZE)
        loads.append((key_ref.at[:, lanes], kv_weight.at[h, :, 0:HEAD_SIZE]))
        loads.append((value_ref.at[:, lanes], kv_weight.at[h, :, HEAD_SIZE : 2 * HEAD_SIZE]))
    kv_loads = len(loads)
    for i, ref in enumerate((query_ref, outer_ref, inner_ref, conv_ref)):
        loads.append((ref, in_weight.at[i]))
    loads.append((tokens_ref, tok.at[:, aligned(me, feat)]))
    token_loads = len(loads)
    for b, ref in enumerate((conv_out_ref, memory_out_ref)):
        for h in range(heads):
            loads.append(
                (
                    ref.at[h * HEAD_SIZE : (h + 1) * HEAD_SIZE, :],
                    out_weight.at[b, h, aligned(me, HEAD_SIZE), :],
                )
            )
    loads = [pltpu.make_async_copy(s, d, load_sem.at[i]) for i, (s, d) in enumerate(loads)]
    store_loads = [
        pltpu.make_async_copy(
            store_ref.at[i * piece : (i + 1) * piece, :],
            passages.at[i * piece : (i + 1) * piece, :],
            store_sem.at[i],
        )
        for i in range(pieces)
    ]
    for copy in loads[:kv_loads] + store_loads + loads[kv_loads:]:
        copy.start()

    barrier = pltpu.get_barrier_semaphore()
    for m in range(1, owners):
        pl.semaphore_signal(barrier, inc=1, device_id=(flip(st, m), me), device_id_type=MESH)
    for d in range(1, team):
        pl.semaphore_signal(
            barrier, inc=1, device_id=(st, lax.rem(me + d, team)), device_id_type=MESH
        )
    pl.semaphore_wait(barrier, owners - 1 + team - 1)

    def remote(src, dst, send, recv, device):
        return pltpu.make_async_remote_copy(
            src_ref=src,
            dst_ref=dst,
            send_sem=send,
            recv_sem=recv,
            device_id=device,
            device_id_type=MESH,
        )

    def ask(m, slot):
        return remote(
            ask_ref.at[flip(st, m)],
            wanted.at[slot],
            ask_send.at[m],
            ask_recv.at[m],
            (flip(st, m), me),
        )

    for m in range(owners - 1, 0, -1):
        ask(m, st).start()

    def far_copy(k, c, owner):
        return remote(
            tokens_ref.at[aligned(c, SEQ_LEN), :],
            tok.at[aligned(c, SEQ_LEN), aligned(owner, feat)],
            far_send.at[k - 1, c],
            far_recv.at[k - 1, c],
            (st, up(k)),
        )

    def near_copy(c, owner):
        return remote(
            tokens_ref.at[aligned(c, SEQ_LEN), :],
            tok.at[aligned(c, SEQ_LEN), aligned(owner, feat)],
            near_send.at[c],
            near_recv.at[c],
            (st, partner),
        )

    def pass_copy(k, c, owner):
        place = tok.at[aligned(c, SEQ_LEN), aligned(owner, feat)]
        return remote(
            place, place, pass_send.at[k - 1, c], pass_recv.at[k - 1, c], (st, partner)
        )

    @pl.loop(0, chunks)
    def _(c):
        for k in range(1, chips):
            far_copy(k, c, me).start()
        near_copy(c, me).start()

    def serve(h, m, slot):
        return remote(
            staged[h].at[flip(st, m)],
            served[h].at[aligned(slot, capacity)],
            serve_send.at[h, m],
            serve_recv.at[h, m],
            (flip(st, m), me),
        )

    for h in range(heads):
        loads[2 * h].wait()
        loads[2 * h + 1].wait()
        for i in range(pieces):
            if h == 0:
                store_loads[i].wait()
            found = jnp.dot(
                passages[i * piece : (i + 1) * piece, :],
                kv_weight[h],
                preferred_element_type=jnp.float32,
            ).astype(jnp.bfloat16)
            count = piece // PLEN
            table[h][i * count : (i + 1) * count] = found.reshape(count, PLEN, 2 * HEAD_SIZE)
        if h == 0:
            for m in range(1, owners):
                ask(m, flip(st, m)).wait_recv()
            numbers = pltpu.make_async_copy(wanted, wanted_smem, smem_sem)
            numbers.start()
            numbers.wait()
        for m in range(owners - 1, 0, -1):
            reader = flip(st, m)
            for c in range(capacity):
                staged[h][reader, c] = table[h][wanted_smem[reader, 0, c]]
            if m < owners - 1:
                serve(h, m + 1, st).start()
        for c in range(capacity):
            served[h][st * capacity + c] = table[h][mine_ref[st * capacity + c]]
        serve(h, 1, st).start()

    def w_near(owner):
        place = out_weight.at[:, :, aligned(owner, HEAD_SIZE), :]
        return remote(place, place, w_near_send, w_near_recv, (st, partner))

    def w_far(k, owner):
        place = out_weight.at[half, :, aligned(owner, HEAD_SIZE), :]
        return remote(place, place, w_far_send.at[k - 1], w_far_recv.at[k - 1], (st, up(k)))

    def w_side(k, owner, which):
        place = out_weight.at[which, :, aligned(owner, HEAD_SIZE), :]
        return remote(place, place, w_side_send.at[k - 1], w_side_recv.at[k - 1], (side, me))

    def w_pass(j, k, owner, which):
        place = out_weight.at[which, :, aligned(owner, HEAD_SIZE), :]
        return remote(
            place, place, w_pass_send.at[j, k - 1], w_pass_recv.at[j, k - 1], (st, partner)
        )

    for copy in loads[kv_loads:]:
        copy.wait()
    for k in range(1, chips):
        w_far(k, me).start()
    w_near(me).start()

    row_number = lax.broadcasted_iota(jnp.int32, (SEQ_LEN, 1), 0)
    taps = taps_ref[...].astype(jnp.float32)

    @pl.loop(0, chunks)
    def _(c):
        for k in range(1, chips):
            far_copy(k, c, down(k)).wait_recv()
            pass_copy(k, c, down(k)).start()
        near_copy(c, partner).wait_recv()
        for k in range(1, chips):
            pass_copy(k, c, down_other(k)).wait_recv()
        here = aligned(c, SEQ_LEN)
        x = tok[here, :]
        dot = functools.partial(jnp.dot, preferred_element_type=jnp.float32)
        queries[here, :] = dot(x, in_weight[0]).astype(jnp.bfloat16)
        mixed = dot(x, in_weight[2]) * dot(x, in_weight[3])
        filtered = jnp.zeros_like(mixed)
        for offset in range(CONV_K):
            back = CONV_K - 1 - offset
            shifted = mixed
            if back:
                shifted = jnp.where(row_number >= back, pltpu.roll(mixed, back, 0), 0.0)
            filtered = filtered + taps[offset : offset + 1, :] * shifted
        conv = (dot(x, in_weight[1]) * filtered).astype(jnp.bfloat16)
        for h in range(heads):
            branch[h][here, :] = conv[:, h * HEAD_SIZE : (h + 1) * HEAD_SIZE]

    def row_copy(i, d, source):
        owner = lax.rem(me + d, team)
        return remote(
            branch[i].at[aligned(owner, own_rows), :],
            moved[i].at[:, aligned(source, HEAD_SIZE)],
            row_send.at[i, d],
            row_recv.at[i, d],
            (st, owner),
        )

    def keep_rows(i):
        moved[i][:, aligned(me, HEAD_SIZE)] = branch[i][aligned(me, own_rows), :]

    def wait_rows(i):
        for d in range(1, team):
            row_copy(i, d, lax.rem(me + team - d, team)).wait_recv()

    for i in range(heads):
        for d in range(1, team):
            row_copy(i, d, me).start()
        keep_rows(i)

    gates[...] = jax.nn.sigmoid(
        jnp.dot(tok[aligned(me, own_rows), :], gate_ref[...], preferred_element_type=jnp.float32)
    )

    order = [d for d in range(1, team) if d % CORES == 0]
    order += [d for d in range(1, team) if d % CORES]
    blocks = own_rows // BLOCK
    tile = 512
    tiles = out_weight.shape[3] // tile

    def attention(h):
        for m in range(1, owners):
            serve(h, m, flip(st, m)).wait_recv()

        def owner_rows(d):
            owner = lax.rem(me + d, team)
            for b in range(blocks):
                number = owner * blocks + b
                here = aligned(number, BLOCK)
                joined = jnp.concatenate(
                    [served[h][target_ref[number * NPB + j]] for j in range(NPB)], axis=0
                )
                scores = lax.dot_general(
                    queries[here, h * HEAD_SIZE : (h + 1) * HEAD_SIZE],
                    joined[:, :HEAD_SIZE],
                    (((1,), (1,)), ((), ())),
                    preferred_element_type=jnp.float32,
                ) * HEAD_SIZE ** (-0.5)
                scores = jnp.exp(scores - jnp.max(scores, axis=1, keepdims=True))
                weights = (scores / jnp.sum(scores, axis=1, keepdims=True)).astype(jnp.bfloat16)
                branch[heads + h][here, :] = jnp.dot(
                    weights, joined[:, HEAD_SIZE:], preferred_element_type=jnp.float32
                ).astype(jnp.bfloat16)

        for d in order:
            owner_rows(d)
            row_copy(heads + h, d, me).start()
        owner_rows(0)
        keep_rows(heads + h)

    for h in range(heads):
        attention(h)
        if h == 0:
            for k in range(1, chips):
                w_far(k, down(k)).wait_recv()
                w_side(k, down(k), half).start()
                w_pass(0, k, down(k), half).start()
            for k in range(1, chips):
                w_side(k, down(k), 1 - half).wait_recv()
                w_pass(1, k, down(k), 1 - half).start()
            w_near(partner).wait_recv()
            for k in range(1, chips):
                w_pass(0, k, down_other(k), half).wait_recv()
                w_pass(1, k, down_other(k), 1 - half).wait_recv()
            for i in range(heads):
                wait_rows(i)

            @pl.loop(0, tiles)
            def _(n):
                lanes = aligned(n, tile)
                value = 0.0
                for i in range(heads):
                    value = value + jnp.dot(
                        moved[i][...],
                        out_weight[0, i, :, lanes],
                        preferred_element_type=jnp.float32,
                    )
                total[:, lanes] = gates[:, 0:1] * value

        wait_rows(heads + h)

        @pl.loop(0, tiles)
        def _(n):
            lanes = aligned(n, tile)
            value = total[:, lanes] + gates[:, 1:2] * jnp.dot(
                moved[heads + h][...],
                out_weight[1, h, :, lanes],
                preferred_element_type=jnp.float32,
            )
            if h < heads - 1:
                total[:, lanes] = value
            else:
                result[:, lanes] = value.astype(jnp.bfloat16)

    written = pltpu.make_async_copy(result, out_ref, out_sem)
    written.start()

    for m in range(1, owners):
        ask(m, st).wait_send()
        for h in range(heads):
            serve(h, m, st).wait_send()

    @pl.loop(0, chunks)
    def _(c):
        for k in range(1, chips):
            far_copy(k, c, me).wait_send()
            pass_copy(k, c, down(k)).wait_send()
        near_copy(c, me).wait_send()

    for k in range(1, chips):
        w_far(k, me).wait_send()
        w_side(k, down(k), half).wait_send()
        w_pass(0, k, down(k), half).wait_send()
        w_pass(1, k, down(k), 1 - half).wait_send()
    w_near(me).wait_send()
    for i in range(2 * heads):
        for d in range(1, team):
            row_copy(i, d, me).wait_send()
    written.wait()


def local(
    tokens,
    store,
    passage_holder_index,
    passage_slot,
    query_weight,
    key_matrix,
    value_weight,
    outer_gate,
    inner_gate,
    conv_input,
    conv_taps,
    route_gate_projection,
    conv_out,
    memory_out,
):
    rows, feat = tokens.shape
    head_width = query_weight.shape[1]
    heads = head_width // HEAD_SIZE
    width = conv_out.shape[1]
    team = lax.axis_size("tp")
    owners = lax.axis_size("st")
    own_rows = rows // team
    depth = team * HEAD_SIZE
    chips = team // CORES
    chunks = rows // SEQ_LEN

    names = passage_holder_index.reshape(-1)
    slots = passage_slot.reshape(-1)
    count = names.shape[0]
    capacity = max(2, 2 * count // owners)
    earlier = jnp.arange(count)[None, :] < jnp.arange(count)[:, None]
    position = jnp.sum(
        jnp.where(earlier & (names[:, None] == names[None, :]), 1, 0), axis=1, dtype=jnp.int32
    )
    target = names * capacity + position
    places = jnp.arange(owners * capacity, dtype=jnp.int32)
    mine = jnp.sum(
        jnp.where(target[None, :] == places[:, None], slots[None, :], 0), axis=1, dtype=jnp.int32
    )
    ask = jnp.pad(mine.reshape(owners, 1, capacity), ((0, 0), (0, 7), (0, LANES - capacity)))
    gate_weight = jnp.pad(route_gate_projection, ((0, 0), (0, LANES - 2)))

    flat_rows = store.reshape(-1, store.shape[-1])
    held = store.shape[0]
    bf16, f32 = jnp.bfloat16, jnp.float32
    dma = pltpu.SemaphoreType.DMA
    scratch = [
        pltpu.VMEM((rows, team * feat), bf16),
        pltpu.VMEM(flat_rows.shape, bf16),
        pltpu.VMEM((4, team * feat, head_width), bf16),
        pltpu.VMEM((heads, team * feat, 2 * HEAD_SIZE), bf16),
        pltpu.VMEM((2, heads, depth, width), bf16),
        pltpu.VMEM((own_rows, width), f32),
        pltpu.VMEM((rows, head_width), bf16),
        pltpu.VMEM((own_rows, LANES), f32),
        pltpu.VMEM((own_rows, width), bf16),
        pltpu.VMEM((owners, 8, LANES), jnp.int32),
        pltpu.SMEM((owners, 8, LANES), jnp.int32),
    ]
    scratch += [pltpu.VMEM((held, PLEN, 2 * HEAD_SIZE), bf16)] * heads
    scratch += [pltpu.VMEM((owners, capacity, PLEN, 2 * HEAD_SIZE), bf16)] * heads
    scratch += [pltpu.VMEM((owners * capacity, PLEN, 2 * HEAD_SIZE), bf16)] * heads
    scratch += [pltpu.VMEM((rows, HEAD_SIZE), bf16)] * (2 * heads)
    scratch += [pltpu.VMEM((own_rows, depth), bf16)] * (2 * heads)
    scratch += [
        dma((4 * heads + 5,)),
        dma((4,)),
        dma,
        dma((owners,)),
        dma((owners,)),
        dma((chunks,)),
        dma((chunks,)),
        dma((chips - 1, chunks)),
        dma((chips - 1, chunks)),
        dma((chips - 1, chunks)),
        dma((chips - 1, chunks)),
        dma((heads, owners)),
        dma((heads, owners)),
        dma((2 * heads, team)),
        dma((2 * heads, team)),
        dma,
        dma,
        dma((chips - 1,)),
        dma((chips - 1,)),
        dma((chips - 1,)),
        dma((chips - 1,)),
        dma((2, chips - 1)),
        dma((2, chips - 1)),
        dma,
    ]
    smem = pl.BlockSpec(memory_space=pltpu.SMEM)
    vmem = pl.BlockSpec(memory_space=pltpu.VMEM)
    hbm = pl.BlockSpec(memory_space=pl.ANY)
    return pl.pallas_call(
        functools.partial(fused_kernel, (owners, team, heads, capacity, rows, feat)),
        out_shape=jax.ShapeDtypeStruct((own_rows, width), bf16),
        in_specs=[smem, smem, vmem] + [hbm] * 8 + [vmem, vmem] + [hbm] * 2,
        out_specs=hbm,
        scratch_shapes=scratch,
        compiler_params=pltpu.CompilerParams(
            collective_id=0, has_side_effects=True, vmem_limit_bytes=66_000_000
        ),
    )(
        target,
        mine,
        ask,
        tokens,
        flat_rows,
        key_matrix,
        value_weight,
        query_weight,
        outer_gate,
        inner_gate,
        conv_input,
        conv_taps,
        gate_weight,
        conv_out,
        memory_out,
    )


def solution(mesh):
    return jax.shard_map(
        local,
        mesh=mesh,
        in_specs=(
            P("st", "tp"),
            P("st", None, None),
            P("st", None),
            P("st", None),
            P(None, "tp"),
            P(None, "tp"),
            P(None, "tp"),
            P(None, "tp"),
            P(None, "tp"),
            P(None, "tp"),
            P(None, "tp"),
            P(),
            P("tp", None),
            P("tp", None),
        ),
        out_specs=P(("st", "tp"), None),
        check_vma=False,
    )
```

```python
import functools

import jax
import jax.numpy as jnp
from jax import lax
from jax.experimental import pallas as pl
from jax.experimental.pallas import tpu as pltpu
from jax.sharding import PartitionSpec as P

HEAD_SIZE = 128
CONV_K = 3
SEQ_LEN = 256
BLOCK = 128
NPB = 2
PLEN = 64
CORES = 2
LANES = 128
LOG2_E = 1.4426950408889634
MESH = pl.DeviceIdType.MESH


def flip(index, mask):
    result, bit = index, 1
    while bit <= mask:
        if mask & bit:
            result = result + bit * (1 - 2 * ((index // bit) % 2))
        bit *= 2
    return result


def aligned(start, size):
    return pl.ds(pl.multiple_of(start * size, size), size)


def fused_kernel(
    sizes,
    names_ref,
    slots_ref,
    tokens_ref,
    store_ref,
    key_ref,
    value_ref,
    query_ref,
    outer_ref,
    inner_ref,
    conv_ref,
    taps_ref,
    gate_ref,
    conv_out_ref,
    memory_out_ref,
    out_ref,
    tok,
    passages,
    in_weight,
    kv_weight,
    out_weight,
    total,
    queries,
    gates,
    powers,
    asked,
    wanted,
    target,
    *rest,
):
    owners, team, heads, capacity, rows, feat = sizes
    chips = team // CORES
    own_rows = rows // team
    chunks = rows // SEQ_LEN
    refs = iter(rest)
    table = [next(refs) for _ in range(2 * heads)]
    staged = [next(refs) for _ in range(2 * heads)]
    served = [next(refs) for _ in range(2 * heads)]
    branch = [next(refs) for _ in range(2 * heads)]
    moved = [next(refs) for _ in range(2 * heads)]
    (
        load_sem,
        store_sem,
        smem_sem,
        ask_send,
        ask_recv,
        near_send,
        near_recv,
        far_send,
        far_recv,
        pass_send,
        pass_recv,
        serve_send,
        serve_recv,
        row_send,
        row_recv,
        w_near_send,
        w_near_recv,
        w_far_send,
        w_far_recv,
        w_side_send,
        w_side_recv,
        w_pass_send,
        w_pass_recv,
    ) = refs

    st = lax.axis_index("st")
    me = lax.axis_index("tp")
    chip, core = me // CORES, me % CORES
    partner = chip * CORES + 1 - core
    side = flip(st, 1)
    half = st % 2

    def up(k):
        return lax.rem(chip + k, chips) * CORES + core

    def down(k):
        return lax.rem(chip + chips - k, chips) * CORES + core

    def down_other(k):
        return lax.rem(chip + chips - k, chips) * CORES + 1 - core

    passage_rows = passages.shape[0]
    pieces = 4
    piece = passage_rows // pieces
    loads = []
    for h in range(heads):
        lanes = slice(h * HEAD_SIZE, (h + 1) * HEAD_SIZE)
        loads.append((key_ref.at[:, lanes], kv_weight.at[h, :, 0:HEAD_SIZE]))
        loads.append((value_ref.at[:, lanes], kv_weight.at[h, :, HEAD_SIZE : 2 * HEAD_SIZE]))
    kv_loads = len(loads)
    for i, ref in enumerate((query_ref, outer_ref, inner_ref, conv_ref)):
        loads.append((ref, in_weight.at[i]))
    loads.append((tokens_ref, tok.at[:, aligned(me, feat)]))
    token_loads = len(loads)
    for b, ref in enumerate((conv_out_ref, memory_out_ref)):
        for h in range(heads):
            loads.append(
                (
                    ref.at[h * HEAD_SIZE : (h + 1) * HEAD_SIZE, :],
                    out_weight.at[b, h, aligned(me, HEAD_SIZE), :],
                )
            )
    loads = [pltpu.make_async_copy(s, d, load_sem.at[i]) for i, (s, d) in enumerate(loads)]
    store_loads = [
        pltpu.make_async_copy(
            store_ref.at[i * piece : (i + 1) * piece, :],
            passages.at[i * piece : (i + 1) * piece, :],
            store_sem.at[i],
        )
        for i in range(pieces)
    ]
    for copy in loads[:2] + store_loads + loads[token_loads:]:
        copy.start()

    barrier = pltpu.get_barrier_semaphore()
    for m in range(1, owners):
        pl.semaphore_signal(barrier, inc=1, device_id=(flip(st, m), me), device_id_type=MESH)
    for d in range(1, team):
        pl.semaphore_signal(
            barrier, inc=1, device_id=(st, lax.rem(me + d, team)), device_id_type=MESH
        )

    lane = lax.broadcasted_iota(jnp.int32, (owners, LANES), 1)
    row = lax.broadcasted_iota(jnp.int32, (owners, LANES), 0)
    requests = [(j, b) for j in range(NPB) for b in range(names_ref.shape[1])]
    filled = jnp.zeros((owners, LANES), jnp.int32)
    asks = jnp.zeros((owners, LANES), jnp.int32)
    for j, b in requests:
        hit = row == names_ref[j, b]
        asks = jnp.where(hit & (lane == filled), slots_ref[j, b], asks)
        filled = jnp.where(hit, filled + 1, filled)
    for o in range(owners):
        asked[o, 0:1, :] = asks[o : o + 1, :]

    def project(h, i):
        found = jnp.dot(
            passages[i * piece : (i + 1) * piece, :],
            kv_weight[h],
            preferred_element_type=jnp.float32,
        ).astype(jnp.bfloat16)
        count = piece // PLEN
        for j in range(2):
            part = found[:, j * HEAD_SIZE : (j + 1) * HEAD_SIZE]
            table[2 * h + j][i * count : (i + 1) * count] = part.reshape(count, PLEN, HEAD_SIZE)

    def project_half(part):
        mine = range(part * pieces // 2, (part + 1) * pieces // 2)
        for i in mine:
            store_loads[i].wait()
        for i in mine:
            project(0, i)

    pl.semaphore_wait(barrier, owners - 1 + team - 1)

    def remote(src, dst, send, recv, device):
        return pltpu.make_async_remote_copy(
            src_ref=src,
            dst_ref=dst,
            send_sem=send,
            recv_sem=recv,
            device_id=device,
            device_id_type=MESH,
        )

    def ask(m, slot):
        return remote(
            asked.at[flip(st, m)],
            wanted.at[slot],
            ask_send.at[m],
            ask_recv.at[m],
            (flip(st, m), me),
        )

    for m in range(owners - 1, 0, -1):
        ask(m, st).start()
    loads[0].wait()
    loads[1].wait()
    project_half(0)

    def far_copy(k, c, owner):
        return remote(
            tokens_ref.at[aligned(c, SEQ_LEN), :],
            tok.at[aligned(c, SEQ_LEN), aligned(owner, feat)],
            far_send.at[k - 1, c],
            far_recv.at[k - 1, c],
            (st, up(k)),
        )

    def near_copy(c, owner):
        return remote(
            tokens_ref.at[aligned(c, SEQ_LEN), :],
            tok.at[aligned(c, SEQ_LEN), aligned(owner, feat)],
            near_send.at[c],
            near_recv.at[c],
            (st, partner),
        )

    def pass_copy(k, c, owner):
        place = tok.at[aligned(c, SEQ_LEN), aligned(owner, feat)]
        return remote(
            place, place, pass_send.at[k - 1, c], pass_recv.at[k - 1, c], (st, partner)
        )

    def w_near(owner):
        place = out_weight.at[:, :, aligned(owner, HEAD_SIZE), :]
        return remote(place, place, w_near_send, w_near_recv, (st, partner))

    def w_far(k, owner):
        place = out_weight.at[half, :, aligned(owner, HEAD_SIZE), :]
        return remote(place, place, w_far_send.at[k - 1], w_far_recv.at[k - 1], (st, up(k)))

    def w_side(k, owner, which):
        place = out_weight.at[which, :, aligned(owner, HEAD_SIZE), :]
        return remote(place, place, w_side_send.at[k - 1], w_side_recv.at[k - 1], (side, me))

    def w_pass(j, k, owner, which):
        place = out_weight.at[which, :, aligned(owner, HEAD_SIZE), :]
        return remote(
            place, place, w_pass_send.at[j, k - 1], w_pass_recv.at[j, k - 1], (st, partner)
        )

    for copy in loads[token_loads:]:
        copy.wait()
    for k in range(1, chips):
        w_far(k, me).start()
    w_near(me).start()

    @pl.loop(0, chunks)
    def _(c):
        for k in range(1, chips):
            far_copy(k, c, me).start()
        near_copy(c, me).start()

    def serve(i, m, slot):
        return remote(
            staged[i].at[flip(st, m)],
            served[i].at[aligned(slot, capacity)],
            serve_send.at[i, m],
            serve_recv.at[i, m],
            (flip(st, m), me),
        )

    def pass_weights():
        for k in range(1, chips):
            w_far(k, down(k)).wait_recv()
            w_side(k, down(k), half).start()
            w_pass(0, k, down(k), half).start()

    project_half(1)
    for copy in loads[2:token_loads]:
        copy.start()
    own_asks = pltpu.make_async_copy(asked.at[st], wanted.at[st], smem_sem)
    own_asks.start()
    for m in range(1, owners):
        ask(m, flip(st, m)).wait_recv()
    own_asks.wait()
    for h in range(heads):
        if h:
            loads[2 * h].wait()
            loads[2 * h + 1].wait()
            for i in range(pieces):
                project(h, i)
        if h == 1:
            pass_weights()
        for i in (2 * h, 2 * h + 1):
            for m in range(owners - 1, 0, -1):
                reader = flip(st, m)
                for c in range(capacity):
                    staged[i][reader, c] = table[i][wanted[reader, 0, c]]
                if m < owners - 1:
                    serve(i, m + 1, st).start()
            for c in range(capacity):
                served[i][st * capacity + c] = table[i][wanted[st, 0, c]]
            serve(i, 1, st).start()
    if heads == 1:
        pass_weights()

    for f, (j, b) in enumerate(requests):
        name = names_ref[j, b]
        place = name * capacity
        for i, a in requests[:f]:
            place = place + jnp.where(names_ref[i, a] == name, 1, 0)
        target[b * NPB + j] = place

    for copy in loads[kv_loads:token_loads]:
        copy.wait()

    row_number = lax.broadcasted_iota(jnp.int32, (SEQ_LEN, 1), 0)
    taps = taps_ref[...].astype(jnp.float32)

    @pl.loop(0, chunks)
    def _(c):
        for k in range(1, chips):
            far_copy(k, c, down(k)).wait_recv()
            pass_copy(k, c, down(k)).start()
        near_copy(c, partner).wait_recv()
        for k in range(1, chips):
            pass_copy(k, c, down_other(k)).wait_recv()
        here = aligned(c, SEQ_LEN)
        x = tok[here, :]
        dot = functools.partial(jnp.dot, preferred_element_type=jnp.float32)
        queries[here, :] = dot(x, in_weight[0]).astype(jnp.bfloat16)
        mixed = dot(x, in_weight[2]) * dot(x, in_weight[3])
        filtered = jnp.zeros_like(mixed)
        for offset in range(CONV_K):
            back = CONV_K - 1 - offset
            shifted = mixed
            if back:
                shifted = jnp.where(row_number >= back, pltpu.roll(mixed, back, 0), 0.0)
            filtered = filtered + taps[offset : offset + 1, :] * shifted
        conv = (dot(x, in_weight[1]) * filtered).astype(jnp.bfloat16)
        for h in range(heads):
            branch[h][here, :] = conv[:, h * HEAD_SIZE : (h + 1) * HEAD_SIZE]

    others = [place(k) for k in range(1, chips) for place in (down, down_other)] + [partner]

    def row_send_copy(i, owner):
        d = lax.rem(owner - me + team, team)
        return remote(
            branch[i].at[aligned(owner, own_rows), :],
            moved[i].at[:, aligned(me, HEAD_SIZE)],
            row_send.at[i, d],
            row_recv.at[i, d],
            (st, owner),
        )

    def row_recv_copy(i, source):
        d = lax.rem(me - source + team, team)
        return remote(
            branch[i].at[aligned(source, own_rows), :],
            moved[i].at[:, aligned(source, HEAD_SIZE)],
            row_send.at[i, d],
            row_recv.at[i, d],
            (st, source),
        )

    def keep_rows(i):
        moved[i][:, aligned(me, HEAD_SIZE)] = branch[i][aligned(me, own_rows), :]

    def wait_rows(i):
        for source in others:
            row_recv_copy(i, source).wait_recv()

    for i in range(heads):
        for owner in others:
            row_send_copy(i, owner).start()
        keep_rows(i)

    gates[...] = jax.nn.sigmoid(
        lax.dot_general(
            tok[aligned(me, own_rows), :],
            gate_ref[...],
            (((1,), (1,)), ((), ())),
            preferred_element_type=jnp.float32,
        )
    )

    blocks = own_rows // BLOCK
    tile = 512
    tiles = out_weight.shape[3] // tile

    ones = jnp.ones((NPB * PLEN, HEAD_SIZE), jnp.bfloat16)

    def attention(h):
        def owner_powers(owner):
            for b in range(blocks):
                n = owner * blocks + b
                keys = jnp.concatenate(
                    [served[2 * h][target[n * NPB + j]] for j in range(NPB)], axis=0
                )
                scores = lax.dot_general(
                    queries[aligned(n, BLOCK), h * HEAD_SIZE : (h + 1) * HEAD_SIZE],
                    keys,
                    (((1,), (1,)), ((), ())),
                    preferred_element_type=jnp.float32,
                )
                scores = scores - jnp.max(scores, axis=1, keepdims=True)
                powers[aligned(n, BLOCK), :] = jnp.exp2(
                    scores * (HEAD_SIZE**-0.5 * LOG2_E)
                ).astype(jnp.bfloat16)

        def owner_rows(owner):
            numbers = [owner * blocks + b for b in range(blocks)]
            values = [
                jnp.concatenate(
                    [served[2 * h + 1][target[n * NPB + j]] for j in range(NPB)], axis=0
                )
                for n in numbers
            ]
            sums = [
                jnp.dot(
                    powers[aligned(n, BLOCK), :],
                    jnp.concatenate([value, ones], axis=1),
                    preferred_element_type=jnp.float32,
                )
                for n, value in zip(numbers, values)
            ]
            for n, both in zip(numbers, sums):
                branch[heads + h][aligned(n, BLOCK), :] = (
                    both[:, :HEAD_SIZE] / both[:, HEAD_SIZE:]
                ).astype(jnp.bfloat16)

        for m in range(1, owners):
            serve(2 * h, m, flip(st, m)).wait_recv()

        @pl.loop(0, team)
        def _(owner):
            owner_powers(owner)

        for m in range(1, owners):
            serve(2 * h + 1, m, flip(st, m)).wait_recv()
        for owner in others:
            owner_rows(owner)
            row_send_copy(heads + h, owner).start()
        owner_rows(me)
        keep_rows(heads + h)

    def add_memory(h, near, far, last):
        def add_tile(n):
            lanes = aligned(n, tile)
            value = total[:, lanes]
            for k in range(0 if near else 1, chips if far else 1):
                rows_of = aligned(lax.rem(chip + k, chips), CORES * HEAD_SIZE)
                value = value + gates[:, 1:2] * jnp.dot(
                    moved[heads + h][:, rows_of],
                    out_weight[1, h, rows_of, lanes],
                    preferred_element_type=jnp.float32,
                )
            if last:
                out_ref[:, lanes] = value.astype(jnp.bfloat16)
            else:
                total[:, lanes] = value

        if last:
            for n in range(tiles):
                add_tile(n)
        else:
            pl.loop(0, tiles)(add_tile)

    for k in range(1, chips):
        w_side(k, down(k), 1 - half).wait_recv()
        w_pass(1, k, down(k), 1 - half).start()

    def drain():
        for m in range(1, owners):
            ask(m, st).wait_send()
            for i in range(2 * heads):
                serve(i, m, st).wait_send()

        @pl.loop(0, chunks)
        def _(c):
            for k in range(1, chips):
                far_copy(k, c, me).wait_send()
                pass_copy(k, c, down(k)).wait_send()
            near_copy(c, me).wait_send()

        for k in range(1, chips):
            w_far(k, me).wait_send()
            w_side(k, down(k), half).wait_send()
            w_pass(0, k, down(k), half).wait_send()
            w_pass(1, k, down(k), 1 - half).wait_send()
        w_near(me).wait_send()

    for h in range(heads):
        attention(h)
        if h == 0:
            w_near(partner).wait_recv()
            for k in range(1, chips):
                w_pass(0, k, down_other(k), half).wait_recv()
                w_pass(1, k, down_other(k), 1 - half).wait_recv()
            for i in range(heads):
                wait_rows(i)

            @pl.loop(0, tiles)
            def _(n):
                lanes = aligned(n, tile)
                value = 0.0
                for i in range(heads):
                    value = value + jnp.dot(
                        moved[i][...],
                        out_weight[0, i, :, lanes],
                        preferred_element_type=jnp.float32,
                    )
                total[:, lanes] = gates[:, 0:1] * value

        if h < heads - 1:
            wait_rows(heads + h)
            add_memory(h, True, True, False)
        else:
            row_recv_copy(heads + h, partner).wait_recv()
            add_memory(h, True, False, False)
            drain()
            for source in others[:-1]:
                row_recv_copy(heads + h, source).wait_recv()
            add_memory(h, False, True, True)

    for i in range(2 * heads):
        for owner in others:
            row_send_copy(i, owner).wait_send()


def local(
    tokens,
    store,
    passage_holder_index,
    passage_slot,
    query_weight,
    key_matrix,
    value_weight,
    outer_gate,
    inner_gate,
    conv_input,
    conv_taps,
    route_gate_projection,
    conv_out,
    memory_out,
):
    rows, feat = tokens.shape
    head_width = query_weight.shape[1]
    heads = head_width // HEAD_SIZE
    width = conv_out.shape[1]
    team = lax.axis_size("tp")
    owners = lax.axis_size("st")
    own_rows = rows // team
    depth = team * HEAD_SIZE
    chips = team // CORES
    chunks = rows // SEQ_LEN

    count = passage_holder_index.size
    capacity = max(2, 2 * count // owners)
    flat_rows = store.reshape(-1, store.shape[-1])
    held = store.shape[0]
    bf16, f32 = jnp.bfloat16, jnp.float32
    dma = pltpu.SemaphoreType.DMA
    scratch = [
        pltpu.VMEM((rows, team * feat), bf16),
        pltpu.VMEM(flat_rows.shape, bf16),
        pltpu.VMEM((4, team * feat, head_width), bf16),
        pltpu.VMEM((heads, team * feat, 2 * HEAD_SIZE), bf16),
        pltpu.VMEM((2, heads, depth, width), bf16),
        pltpu.VMEM((own_rows, width), f32),
        pltpu.VMEM((rows, head_width), bf16),
        pltpu.VMEM((own_rows, 2), f32),
        pltpu.VMEM((rows, NPB * PLEN), bf16),
        pltpu.VMEM((owners, 8, LANES), jnp.int32),
        pltpu.SMEM((owners, 8, LANES), jnp.int32),
        pltpu.SMEM((count,), jnp.int32),
    ]
    scratch += [pltpu.VMEM((held, PLEN, HEAD_SIZE), bf16)] * (2 * heads)
    scratch += [pltpu.VMEM((owners, capacity, PLEN, HEAD_SIZE), bf16)] * (2 * heads)
    scratch += [pltpu.VMEM((owners * capacity, PLEN, HEAD_SIZE), bf16)] * (2 * heads)
    scratch += [pltpu.VMEM((rows, HEAD_SIZE), bf16)] * (2 * heads)
    scratch += [pltpu.VMEM((own_rows, depth), bf16)] * (2 * heads)
    scratch += [
        dma((4 * heads + 5,)),
        dma((4,)),
        dma,
        dma((owners,)),
        dma((owners,)),
        dma((chunks,)),
        dma((chunks,)),
        dma((chips - 1, chunks)),
        dma((chips - 1, chunks)),
        dma((chips - 1, chunks)),
        dma((chips - 1, chunks)),
        dma((2 * heads, owners)),
        dma((2 * heads, owners)),
        dma((2 * heads, team)),
        dma((2 * heads, team)),
        dma,
        dma,
        dma((chips - 1,)),
        dma((chips - 1,)),
        dma((chips - 1,)),
        dma((chips - 1,)),
        dma((2, chips - 1)),
        dma((2, chips - 1)),
    ]
    smem = pl.BlockSpec(memory_space=pltpu.SMEM)
    vmem = pl.BlockSpec(memory_space=pltpu.VMEM)
    hbm = pl.BlockSpec(memory_space=pltpu.HBM)
    return pl.pallas_call(
        functools.partial(fused_kernel, (owners, team, heads, capacity, rows, feat)),
        out_shape=pltpu.VMEM((own_rows, width), bf16),
        in_specs=[smem, smem] + [hbm] * 8 + [vmem, vmem] + [hbm] * 2,
        out_specs=vmem,
        scratch_shapes=scratch,
        compiler_params=pltpu.CompilerParams(
            collective_id=0, has_side_effects=True, vmem_limit_bytes=56 * 1024 * 1024
        ),
    )(
        passage_holder_index.T,
        passage_slot.T,
        tokens,
        flat_rows,
        key_matrix,
        value_weight,
        query_weight,
        outer_gate,
        inner_gate,
        conv_input,
        conv_taps,
        route_gate_projection.T,
        conv_out,
        memory_out,
    )


def solution(mesh):
    return jax.shard_map(
        local,
        mesh=mesh,
        in_specs=(
            P("st", "tp"),
            P("st", None, None),
            P("st", None),
            P("st", None),
            P(None, "tp"),
            P(None, "tp"),
            P(None, "tp"),
            P(None, "tp"),
            P(None, "tp"),
            P(None, "tp"),
            P(None, "tp"),
            P(),
            P("tp", None),
            P("tp", None),
        ),
        out_specs=P(("st", "tp"), None),
        check_vma=False,
    )
```

```python
import functools

import jax
import jax.numpy as jnp
from jax import lax
from jax.experimental import pallas as pl
from jax.experimental.pallas import tpu as pltpu
from jax.sharding import PartitionSpec as P

HEAD_SIZE = 128
CONV_K = 3
SEQ_LEN = 256
BLOCK = 128
NPB = 2
PLEN = 64
CORES = 2
LANES = 128
LOG2_E = 1.4426950408889634
MESH = pl.DeviceIdType.MESH


def flip(index, mask):
    result, bit = index, 1
    while bit <= mask:
        if mask & bit:
            result = result + bit * (1 - 2 * ((index // bit) % 2))
        bit *= 2
    return result


def aligned(start, size):
    return pl.ds(pl.multiple_of(start * size, size), size)


def fused_kernel(
    sizes,
    names_ref,
    slots_ref,
    tokens_ref,
    store_ref,
    key_ref,
    value_ref,
    query_ref,
    outer_ref,
    inner_ref,
    conv_ref,
    taps_ref,
    gate_ref,
    conv_out_ref,
    memory_out_ref,
    out_ref,
    spilled_ref,
    tok,
    passages,
    in_weight,
    kv_weight,
    out_weight,
    total,
    queries,
    gates,
    powers,
    asked,
    wanted,
    target,
    *rest,
):
    owners, team, heads, capacity, direct, extra, rows, feat = sizes
    rest_slots = capacity - direct
    parts = 2 * heads
    chips = team // CORES
    own_rows = rows // team
    chunks = rows // SEQ_LEN
    refs = iter(rest)
    table = [next(refs) for _ in range(2 * heads)]
    staged = [next(refs) for _ in range(2 * heads)]
    served = [next(refs) for _ in range(2 * heads)]
    spill_out = [next(refs) for _ in range(2 * heads)] if extra else None
    spill_in = [next(refs) for _ in range(2 * heads)] if extra else None
    packed = [next(refs) for _ in range(2 * heads)] if extra else None
    branch = [next(refs) for _ in range(2 * heads)]
    moved = [next(refs) for _ in range(2 * heads)]
    (
        load_sem,
        store_sem,
        smem_sem,
        ask_send,
        ask_recv,
        near_send,
        near_recv,
        far_send,
        far_recv,
        pass_send,
        pass_recv,
        serve_send,
        serve_recv,
        row_send,
        row_recv,
        w_near_send,
        w_near_recv,
        w_far_send,
        w_far_recv,
        w_side_send,
        w_side_recv,
        w_pass_send,
        w_pass_recv,
        spill_send,
        spill_recv,
        packed_send,
        packed_recv,
    ) = refs

    st = lax.axis_index("st")
    me = lax.axis_index("tp")
    chip, core = me // CORES, me % CORES
    partner = chip * CORES + 1 - core
    mine_piece = st % parts
    half = st // 4
    beside = 1 - half

    def up(k):
        return lax.rem(chip + k, chips) * CORES + core

    def down(k):
        return lax.rem(chip + chips - k, chips) * CORES + core

    def down_other(k):
        return lax.rem(chip + chips - k, chips) * CORES + 1 - core

    passage_rows = passages.shape[0]
    pieces = 4
    piece = passage_rows // pieces
    loads = []
    for h in range(heads):
        lanes = slice(h * HEAD_SIZE, (h + 1) * HEAD_SIZE)
        loads.append((key_ref.at[:, lanes], kv_weight.at[h, :, 0:HEAD_SIZE]))
        loads.append((value_ref.at[:, lanes], kv_weight.at[h, :, HEAD_SIZE : 2 * HEAD_SIZE]))
    kv_loads = len(loads)
    for i, ref in enumerate((query_ref, outer_ref, inner_ref, conv_ref)):
        loads.append((ref, in_weight.at[i]))
    loads.append((tokens_ref, tok.at[:, aligned(me, feat)]))
    token_loads = len(loads)
    for b, ref in enumerate((conv_out_ref, memory_out_ref)):
        for h in range(heads):
            loads.append(
                (
                    ref.at[h * HEAD_SIZE : (h + 1) * HEAD_SIZE, :],
                    out_weight.at[b * heads + h, aligned(me, HEAD_SIZE), :],
                )
            )
    loads = [pltpu.make_async_copy(s, d, load_sem.at[i]) for i, (s, d) in enumerate(loads)]
    store_loads = [
        pltpu.make_async_copy(
            store_ref.at[i * piece : (i + 1) * piece, :],
            passages.at[i * piece : (i + 1) * piece, :],
            store_sem.at[i],
        )
        for i in range(pieces)
    ]
    for copy in loads[:2] + store_loads + loads[token_loads:]:
        copy.start()

    barrier = pltpu.get_barrier_semaphore()
    for m in range(1, owners):
        pl.semaphore_signal(barrier, inc=1, device_id=(flip(st, m), me), device_id_type=MESH)
    for d in range(1, team):
        pl.semaphore_signal(
            barrier, inc=1, device_id=(st, lax.rem(me + d, team)), device_id_type=MESH
        )

    lane = lax.broadcasted_iota(jnp.int32, (owners, LANES), 1)
    row = lax.broadcasted_iota(jnp.int32, (owners, LANES), 0)
    requests = [(j, b) for j in range(NPB) for b in range(names_ref.shape[1])]
    filled = jnp.zeros((owners, LANES), jnp.int32)
    asks = jnp.zeros((owners, LANES), jnp.int32)
    over = jnp.zeros((owners, LANES), jnp.int32)
    for j, b in requests:
        hit = row == names_ref[j, b]
        asks = jnp.where(hit & (lane == filled), slots_ref[j, b], asks)
        if extra:
            late = jnp.where(hit & (filled >= direct) & (row // 4 != half), 1, 0)
            entry = (row % 4) * (2 * rest_slots) + filled - direct
            entry = jnp.sum(late * entry, axis=0, keepdims=True)
            late = jnp.sum(late, axis=0, keepdims=True)
            asks = jnp.where((late > 0) & (lane == capacity + over), entry, asks)
            over = over + late
        filled = jnp.where(hit, filled + 1, filled)
    asks = jnp.where(lane == LANES - 1, over, asks)
    for o in range(owners):
        asked[o, 0:1, :] = asks[o : o + 1, :]

    def project(h, i):
        found = jnp.dot(
            passages[i * piece : (i + 1) * piece, :],
            kv_weight[h],
            preferred_element_type=jnp.float32,
        ).astype(jnp.bfloat16)
        count = piece // PLEN
        for j in range(2):
            part = found[:, j * HEAD_SIZE : (j + 1) * HEAD_SIZE]
            table[2 * h + j][i * count : (i + 1) * count] = part.reshape(count, PLEN, HEAD_SIZE)

    def project_half(part):
        mine = range(part * pieces // 2, (part + 1) * pieces // 2)
        for i in mine:
            store_loads[i].wait()
        for i in mine:
            project(0, i)

    pl.semaphore_wait(barrier, owners - 1 + team - 1)

    def remote(src, dst, send, recv, device):
        return pltpu.make_async_remote_copy(
            src_ref=src,
            dst_ref=dst,
            send_sem=send,
            recv_sem=recv,
            device_id=device,
            device_id_type=MESH,
        )

    def ask(m, slot):
        return remote(
            asked.at[flip(st, m)],
            wanted.at[slot],
            ask_send.at[m],
            ask_recv.at[m],
            (flip(st, m), me),
        )

    for m in range(owners - 1, 0, -1):
        ask(m, st).start()
    loads[0].wait()
    loads[1].wait()
    project_half(0)

    def far_copy(k, c, owner):
        return remote(
            tokens_ref.at[aligned(c, SEQ_LEN), :],
            tok.at[aligned(c, SEQ_LEN), aligned(owner, feat)],
            far_send.at[k - 1, c],
            far_recv.at[k - 1, c],
            (st, up(k)),
        )

    def near_copy(c, owner):
        return remote(
            tokens_ref.at[aligned(c, SEQ_LEN), :],
            tok.at[aligned(c, SEQ_LEN), aligned(owner, feat)],
            near_send.at[c],
            near_recv.at[c],
            (st, partner),
        )

    def pass_copy(k, c, owner):
        place = tok.at[aligned(c, SEQ_LEN), aligned(owner, feat)]
        return remote(
            place, place, pass_send.at[k - 1, c], pass_recv.at[k - 1, c], (st, partner)
        )

    def w_near(owner):
        place = out_weight.at[:, aligned(owner, HEAD_SIZE), :]
        return remote(place, place, w_near_send, w_near_recv, (st, partner))

    def w_place(which, owner):
        return out_weight.at[which, aligned(owner, HEAD_SIZE), :]

    def w_far(k, owner):
        place = w_place(mine_piece, owner)
        return remote(place, place, w_far_send.at[k - 1], w_far_recv.at[k - 1], (st, up(k)))

    def w_side(m, k, which):
        place = w_place(which, down(k))
        return remote(
            place,
            place,
            w_side_send.at[m, k - 1],
            w_side_recv.at[m, k - 1],
            (flip(st, 1 if m == 3 else m), me),
        )

    def w_piece(m):
        return lax.rem(flip(st, m), parts) if m else mine_piece

    def w_sent(m):
        return w_piece(2) if m == 3 else mine_piece

    def w_turn():
        for k in range(1, chips):
            w_side(2, k, w_piece(2)).wait_recv()
            w_side(3, k, w_sent(3)).start()
            w_pass(2, k, down(k)).start()

    def w_pass(m, k, owner):
        place = w_place(w_piece(m), owner)
        return remote(
            place, place, w_pass_send.at[m, k - 1], w_pass_recv.at[m, k - 1], (st, partner)
        )

    for copy in loads[token_loads:]:
        copy.wait()
    for k in range(1, chips):
        w_far(k, me).start()
    w_near(me).start()

    @pl.loop(0, chunks)
    def _(c):
        for k in range(1, chips):
            far_copy(k, c, me).start()
        near_copy(c, me).start()

    def serve(i, m, slot):
        count = direct if m >= 4 else capacity
        return remote(
            staged[i].at[flip(st, m), 0:count],
            served[i].at[pl.ds(slot * capacity, count)],
            serve_send.at[i, m],
            serve_recv.at[i, m],
            (flip(st, m), me),
        )

    def beside_middle(j):
        return j + 2 * beside + 4 * half

    def spill(i, j):
        return remote(
            spill_out[i].at[j],
            spill_in[i].at[pl.ds((st % 4) * 2 * rest_slots, 2 * rest_slots)],
            spill_send.at[i, j],
            spill_recv.at[i, st % 4],
            (beside_middle(j), me),
        )

    def spill_arrival(i, source):
        return remote(
            spill_out[i].at[0],
            spill_in[i].at[pl.ds(source * 2 * rest_slots, 2 * rest_slots)],
            spill_send.at[i, 0],
            spill_recv.at[i, source],
            (source + 4 * half, me),
        )

    def far_reader(j, t):
        return j + 2 * t + 4 * beside

    def start_spill(i):
        for j in range(2):
            here = beside_middle(j) == st
            for t in range(2):
                for c in range(rest_slots):
                    found = table[i][wanted[far_reader(j, t), 0, direct + c]]
                    spill_out[i][j, t * rest_slots + c] = found

            @pl.when(here)
            def _():
                for n in range(2 * rest_slots):
                    spill_in[i][(st % 4) * 2 * rest_slots + n] = spill_out[i][j, n]

            @pl.when(jnp.logical_not(here))
            def _():
                spill(i, j).start()

    def packed_copy(i, t):
        return remote(
            packed[i].at[t],
            served[i].at[pl.ds(owners * capacity, extra)],
            packed_send.at[i, t],
            packed_recv.at[i],
            (far_reader(st % 2, t), me),
        )

    is_beside = (st // 2) % 2 == beside

    def relay(i):
        @pl.when(is_beside)
        def _():
            for source in range(4):

                @pl.when(source != st % 4)
                def _():
                    spill_arrival(i, source).wait_recv()

            for t in range(2):
                for n in range(extra):
                    entry = wanted[far_reader(st % 2, t), 0, capacity + n]
                    packed[i][t, n] = spill_in[i][entry + t * rest_slots]
            for t in range(2):
                packed_copy(i, t).start()

    def wait_served(i):
        for m in range(1, owners):
            serve(i, m, flip(st, m)).wait_recv()
        if extra:
            packed_copy(i, 0).wait_recv()

    def pass_weights():
        for k in range(1, chips):
            w_far(k, down(k)).wait_recv()
            for m in range(1, min(parts, 3)):
                w_side(m, k, mine_piece).start()
            w_pass(0, k, down(k)).start()

    project_half(1)
    for copy in loads[2:token_loads]:
        copy.start()
    own_asks = pltpu.make_async_copy(asked.at[st], wanted.at[st], smem_sem)
    own_asks.start()
    for m in range(1, owners):
        ask(m, flip(st, m)).wait_recv()
    own_asks.wait()
    for h in range(heads):
        if h:
            loads[2 * h].wait()
            loads[2 * h + 1].wait()
            for i in range(pieces):
                project(h, i)
        if extra:
            for i in (2 * h, 2 * h + 1):
                start_spill(i)
            if h == 1:
                relay(0)
                relay(1)
        if h == 1:
            pass_weights()
        for i in (2 * h, 2 * h + 1):
            for m in range(owners - 1, 0, -1):
                reader = flip(st, m)
                for c in range(direct if m >= 4 else capacity):
                    staged[i][reader, c] = table[i][wanted[reader, 0, c]]
                if m < owners - 1:
                    serve(i, m + 1, st).start()
            for c in range(capacity):
                served[i][st * capacity + c] = table[i][wanted[st, 0, c]]
            serve(i, 1, st).start()
    if heads == 1:
        pass_weights()

    late = jnp.int32(0)
    for f, (j, b) in enumerate(requests):
        name = names_ref[j, b]
        place = jnp.int32(0)
        for i, a in requests[:f]:
            place = place + jnp.where(names_ref[i, a] == name, 1, 0)
        where = name * capacity + place
        if extra:
            is_late = jnp.logical_and(place >= direct, name // 4 != half)
            where = jnp.where(is_late, owners * capacity + jnp.minimum(late, extra - 1), where)
            late = late + jnp.where(is_late, 1, 0)
        target[b * NPB + j] = where
    most = late
    for m in range(1, owners):
        most = jnp.maximum(most, wanted[flip(st, m), 0, LANES - 1])
    spilled_ref[0] = most

    for copy in loads[kv_loads:token_loads]:
        copy.wait()

    turn = chunks - 2
    row_number = lax.broadcasted_iota(jnp.int32, (SEQ_LEN, 1), 0)
    taps = taps_ref[...].astype(jnp.float32)

    @pl.loop(0, chunks)
    def _(c):
        if parts == 4:
            pl.when(c == turn)(w_turn)
        for k in range(1, chips):
            far_copy(k, c, down(k)).wait_recv()
            pass_copy(k, c, down(k)).start()
        near_copy(c, partner).wait_recv()
        for k in range(1, chips):
            pass_copy(k, c, down_other(k)).wait_recv()
        here = aligned(c, SEQ_LEN)
        x = tok[here, :]
        dot = functools.partial(jnp.dot, preferred_element_type=jnp.float32)
        queries[here, :] = dot(x, in_weight[0]).astype(jnp.bfloat16)
        mixed = dot(x, in_weight[2]) * dot(x, in_weight[3])
        filtered = jnp.zeros_like(mixed)
        for offset in range(CONV_K):
            back = CONV_K - 1 - offset
            shifted = mixed
            if back:
                shifted = jnp.where(row_number >= back, pltpu.roll(mixed, back, 0), 0.0)
            filtered = filtered + taps[offset : offset + 1, :] * shifted
        conv = (dot(x, in_weight[1]) * filtered).astype(jnp.bfloat16)
        for h in range(heads):
            branch[h][here, :] = conv[:, h * HEAD_SIZE : (h + 1) * HEAD_SIZE]

    if extra:
        for i in range(2 if heads > 1 else 0, parts):
            relay(i)

    others = [place(k) for k in range(1, chips) for place in (down, down_other)] + [partner]

    def row_send_copy(i, owner):
        d = lax.rem(owner - me + team, team)
        return remote(
            branch[i].at[aligned(owner, own_rows), :],
            moved[i].at[:, aligned(me, HEAD_SIZE)],
            row_send.at[i, d],
            row_recv.at[i, d],
            (st, owner),
        )

    def row_recv_copy(i, source):
        d = lax.rem(me - source + team, team)
        return remote(
            branch[i].at[aligned(source, own_rows), :],
            moved[i].at[:, aligned(source, HEAD_SIZE)],
            row_send.at[i, d],
            row_recv.at[i, d],
            (st, source),
        )

    def keep_rows(i):
        moved[i][:, aligned(me, HEAD_SIZE)] = branch[i][aligned(me, own_rows), :]

    def wait_rows(i):
        for source in others:
            row_recv_copy(i, source).wait_recv()

    for i in range(heads):
        for owner in others:
            row_send_copy(i, owner).start()
        keep_rows(i)

    gates[...] = jax.nn.sigmoid(
        lax.dot_general(
            tok[aligned(me, own_rows), :],
            gate_ref[...],
            (((1,), (1,)), ((), ())),
            preferred_element_type=jnp.float32,
        )
    )

    blocks = own_rows // BLOCK
    tile = 512
    tiles = out_weight.shape[2] // tile

    ones = jnp.ones((NPB * PLEN, HEAD_SIZE), jnp.bfloat16)

    def attention(h):
        def owner_powers(owner):
            for b in range(blocks):
                n = owner * blocks + b
                keys = jnp.concatenate(
                    [served[2 * h][target[n * NPB + j]] for j in range(NPB)], axis=0
                )
                scores = lax.dot_general(
                    queries[aligned(n, BLOCK), h * HEAD_SIZE : (h + 1) * HEAD_SIZE],
                    keys,
                    (((1,), (1,)), ((), ())),
                    preferred_element_type=jnp.float32,
                )
                scores = scores - jnp.max(scores, axis=1, keepdims=True)
                powers[aligned(n, BLOCK), :] = jnp.exp2(
                    scores * (HEAD_SIZE**-0.5 * LOG2_E)
                ).astype(jnp.bfloat16)

        def owner_rows(owner):
            numbers = [owner * blocks + b for b in range(blocks)]
            values = [
                jnp.concatenate(
                    [served[2 * h + 1][target[n * NPB + j]] for j in range(NPB)], axis=0
                )
                for n in numbers
            ]
            sums = [
                jnp.dot(
                    powers[aligned(n, BLOCK), :],
                    jnp.concatenate([value, ones], axis=1),
                    preferred_element_type=jnp.float32,
                )
                for n, value in zip(numbers, values)
            ]
            for n, both in zip(numbers, sums):
                branch[heads + h][aligned(n, BLOCK), :] = (
                    both[:, :HEAD_SIZE] / both[:, HEAD_SIZE:]
                ).astype(jnp.bfloat16)

        wait_served(2 * h)

        @pl.loop(0, team)
        def _(owner):
            owner_powers(owner)

        wait_served(2 * h + 1)
        for owner in others:
            owner_rows(owner)
            row_send_copy(heads + h, owner).start()
        owner_rows(me)
        keep_rows(heads + h)

    def add_memory(h, near, far, last):
        def add_tile(n):
            lanes = aligned(n, tile)
            value = total[:, lanes]
            for k in range(0 if near else 1, chips if far else 1):
                rows_of = aligned(lax.rem(chip + k, chips), CORES * HEAD_SIZE)
                value = value + gates[:, 1:2] * jnp.dot(
                    moved[heads + h][:, rows_of],
                    out_weight[heads + h, rows_of, lanes],
                    preferred_element_type=jnp.float32,
                )
            if last:
                out_ref[:, lanes] = value.astype(jnp.bfloat16)
            else:
                total[:, lanes] = value

        if last:
            for n in range(tiles):
                add_tile(n)
        else:
            pl.loop(0, tiles)(add_tile)

    for k in range(1, chips):
        for m in range(1, parts):
            if m != 2:
                w_side(m, k, w_piece(m)).wait_recv()
                w_pass(m, k, down(k)).start()

    def drain():
        for i in range(parts if extra else 0):
            for j in range(2):

                @pl.when(beside_middle(j) != st)
                def _():
                    spill(i, j).wait_send()

            @pl.when(is_beside)
            def _():
                for t in range(2):
                    packed_copy(i, t).wait_send()

        for m in range(1, owners):
            ask(m, st).wait_send()
            for i in range(2 * heads):
                serve(i, m, st).wait_send()

        @pl.loop(0, chunks)
        def _(c):
            for k in range(1, chips):
                far_copy(k, c, me).wait_send()
                pass_copy(k, c, down(k)).wait_send()
            near_copy(c, me).wait_send()

        for k in range(1, chips):
            w_far(k, me).wait_send()
            for m in range(parts):
                if m:
                    w_side(m, k, w_sent(m)).wait_send()
                w_pass(m, k, down(k)).wait_send()
        w_near(me).wait_send()

    for h in range(heads):
        attention(h)
        if h == 0:
            w_near(partner).wait_recv()
            for k in range(1, chips):
                for m in range(parts):
                    w_pass(m, k, down_other(k)).wait_recv()
            for i in range(heads):
                wait_rows(i)

            @pl.loop(0, tiles)
            def _(n):
                lanes = aligned(n, tile)
                value = 0.0
                for i in range(heads):
                    value = value + jnp.dot(
                        moved[i][...],
                        out_weight[i, :, lanes],
                        preferred_element_type=jnp.float32,
                    )
                total[:, lanes] = gates[:, 0:1] * value

        if h < heads - 1:
            wait_rows(heads + h)
            add_memory(h, True, True, False)
        else:
            row_recv_copy(heads + h, partner).wait_recv()
            add_memory(h, True, False, False)
            drain()
            for source in others[:-1]:
                row_recv_copy(heads + h, source).wait_recv()
            add_memory(h, False, True, True)

    for i in range(2 * heads):
        for owner in others:
            row_send_copy(i, owner).wait_send()


def fused(
    spills,
    tokens,
    store,
    passage_holder_index,
    passage_slot,
    query_weight,
    key_matrix,
    value_weight,
    outer_gate,
    inner_gate,
    conv_input,
    conv_taps,
    route_gate_projection,
    conv_out,
    memory_out,
):
    rows, feat = tokens.shape
    head_width = query_weight.shape[1]
    heads = head_width // HEAD_SIZE
    width = conv_out.shape[1]
    team = lax.axis_size("tp")
    owners = lax.axis_size("st")
    own_rows = rows // team
    depth = team * HEAD_SIZE
    chips = team // CORES
    chunks = rows // SEQ_LEN

    count = passage_holder_index.size
    capacity = max(2, 2 * count // owners)
    direct, extra = capacity, 0
    if spills:
        direct = (5 * capacity + 7) // 8
        extra = count * 3 // 16
    flat_rows = store.reshape(-1, store.shape[-1])
    held = store.shape[0]
    bf16, f32 = jnp.bfloat16, jnp.float32
    dma = pltpu.SemaphoreType.DMA
    scratch = [
        pltpu.VMEM((rows, team * feat), bf16),
        pltpu.VMEM(flat_rows.shape, bf16),
        pltpu.VMEM((4, team * feat, head_width), bf16),
        pltpu.VMEM((heads, team * feat, 2 * HEAD_SIZE), bf16),
        pltpu.VMEM((2 * heads, depth, width), bf16),
        pltpu.VMEM((own_rows, width), f32),
        pltpu.VMEM((rows, head_width), bf16),
        pltpu.VMEM((own_rows, 2), f32),
        pltpu.VMEM((rows, NPB * PLEN), bf16),
        pltpu.VMEM((owners, 8, LANES), jnp.int32),
        pltpu.SMEM((owners, 8, LANES), jnp.int32),
        pltpu.SMEM((count,), jnp.int32),
    ]
    scratch += [pltpu.VMEM((held, PLEN, HEAD_SIZE), bf16)] * (2 * heads)
    scratch += [pltpu.VMEM((owners, capacity, PLEN, HEAD_SIZE), bf16)] * (2 * heads)
    scratch += [pltpu.VMEM((owners * capacity + extra, PLEN, HEAD_SIZE), bf16)] * (2 * heads)
    if spills:
        rest_slots = capacity - direct
        scratch += [pltpu.VMEM((2, 2 * rest_slots, PLEN, HEAD_SIZE), bf16)] * (2 * heads)
        scratch += [pltpu.VMEM((8 * rest_slots, PLEN, HEAD_SIZE), bf16)] * (2 * heads)
        scratch += [pltpu.VMEM((2, extra, PLEN, HEAD_SIZE), bf16)] * (2 * heads)
    scratch += [pltpu.VMEM((rows, HEAD_SIZE), bf16)] * (2 * heads)
    scratch += [pltpu.VMEM((own_rows, depth), bf16)] * (2 * heads)
    scratch += [
        dma((4 * heads + 5,)),
        dma((4,)),
        dma,
        dma((owners,)),
        dma((owners,)),
        dma((chunks,)),
        dma((chunks,)),
        dma((chips - 1, chunks)),
        dma((chips - 1, chunks)),
        dma((chips - 1, chunks)),
        dma((chips - 1, chunks)),
        dma((2 * heads, owners)),
        dma((2 * heads, owners)),
        dma((2 * heads, team)),
        dma((2 * heads, team)),
        dma,
        dma,
        dma((chips - 1,)),
        dma((chips - 1,)),
        dma((2 * heads, chips - 1)),
        dma((2 * heads, chips - 1)),
        dma((2 * heads, chips - 1)),
        dma((2 * heads, chips - 1)),
        dma((2 * heads, 2)),
        dma((2 * heads, 4)),
        dma((2 * heads, 2)),
        dma((2 * heads,)),
    ]
    smem = pl.BlockSpec(memory_space=pltpu.SMEM)
    vmem = pl.BlockSpec(memory_space=pltpu.VMEM)
    hbm = pl.BlockSpec(memory_space=pltpu.HBM)
    return pl.pallas_call(
        functools.partial(fused_kernel, (owners, team, heads, capacity, direct, extra, rows, feat)),
        out_shape=(
            pltpu.VMEM((own_rows, width), bf16),
            jax.ShapeDtypeStruct((1,), jnp.int32),
        ),
        in_specs=[smem, smem] + [hbm] * 8 + [vmem, vmem] + [hbm] * 2,
        out_specs=(vmem, smem),
        scratch_shapes=scratch,
        compiler_params=pltpu.CompilerParams(
            collective_id=int(spills), has_side_effects=True, vmem_limit_bytes=56 * 1024 * 1024
        ),
    )(
        passage_holder_index.T,
        passage_slot.T,
        tokens,
        flat_rows,
        key_matrix,
        value_weight,
        query_weight,
        outer_gate,
        inner_gate,
        conv_input,
        conv_taps,
        route_gate_projection.T,
        conv_out,
        memory_out,
    )


def local(*args):
    count, owners = args[2].size, lax.axis_size("st")
    if owners != 8:
        return fused(False, *args)[0]
    result, most = fused(True, *args)
    return lax.cond(
        most[0] > count * 3 // 16, lambda: fused(False, *args)[0], lambda: result
    )


def solution(mesh):
    return jax.shard_map(
        local,
        mesh=mesh,
        in_specs=(
            P("st", "tp"),
            P("st", None, None),
            P("st", None),
            P("st", None),
            P(None, "tp"),
            P(None, "tp"),
            P(None, "tp"),
            P(None, "tp"),
            P(None, "tp"),
            P(None, "tp"),
            P(None, "tp"),
            P(),
            P("tp", None),
            P("tp", None),
        ),
        out_specs=P(("st", "tp"), None),
        check_vma=False,
    )
```

```python
import functools

import jax
import jax.numpy as jnp
from jax import lax
from jax.experimental import pallas as pl
from jax.experimental.pallas import tpu as pltpu
from jax.sharding import PartitionSpec as P

HEAD_SIZE = 128
CONV_K = 3
SEQ_LEN = 256
BLOCK = 128
NPB = 2
PLEN = 64
CORES = 2
LANES = 128
LOG2_E = 1.4426950408889634
MESH = pl.DeviceIdType.MESH


def flip(index, mask):
    result, bit = index, 1
    while bit <= mask:
        if mask & bit:
            result = result + bit * (1 - 2 * ((index // bit) % 2))
        bit *= 2
    return result


def aligned(start, size):
    return pl.ds(pl.multiple_of(start * size, size), size)


def fused_kernel(
    sizes,
    names_ref,
    slots_ref,
    tokens_ref,
    store_ref,
    key_ref,
    value_ref,
    query_ref,
    outer_ref,
    inner_ref,
    conv_ref,
    taps_ref,
    gate_ref,
    conv_out_ref,
    memory_out_ref,
    out_ref,
    spilled_ref,
    tok,
    passages,
    in_weight,
    kv_weight,
    out_weight,
    total,
    queries,
    gates,
    powers,
    asked,
    wanted,
    target,
    *rest,
):
    owners, team, heads, capacity, direct, extra, rows, feat = sizes
    rest_slots = capacity - direct
    parts = 2 * heads
    chips = team // CORES
    own_rows = rows // team
    chunks = rows // SEQ_LEN
    refs = iter(rest)
    table = [next(refs) for _ in range(2 * heads)]
    staged = [next(refs) for _ in range(2 * heads)]
    served = [next(refs) for _ in range(2 * heads)]
    spill_out = [next(refs) for _ in range(2 * heads)] if extra else None
    spill_in = [next(refs) for _ in range(2 * heads)] if extra else None
    packed = [next(refs) for _ in range(2 * heads)] if extra else None
    branch = [next(refs) for _ in range(2 * heads)]
    moved = [next(refs) for _ in range(2 * heads)]
    (
        load_sem,
        store_sem,
        smem_sem,
        ask_send,
        ask_recv,
        near_send,
        near_recv,
        far_send,
        far_recv,
        pass_send,
        pass_recv,
        serve_send,
        serve_recv,
        row_send,
        row_recv,
        w_near_send,
        w_near_recv,
        w_far_send,
        w_far_recv,
        w_side_send,
        w_side_recv,
        w_pass_send,
        w_pass_recv,
        spill_send,
        spill_recv,
        packed_send,
        packed_recv,
    ) = refs

    st = lax.axis_index("st")
    me = lax.axis_index("tp")
    chip, core = me // CORES, me % CORES
    partner = chip * CORES + 1 - core
    mine_piece = st % parts
    half = st // 4
    beside = 1 - half

    def up(k):
        return lax.rem(chip + k, chips) * CORES + core

    def down(k):
        return lax.rem(chip + chips - k, chips) * CORES + core

    def down_other(k):
        return lax.rem(chip + chips - k, chips) * CORES + 1 - core

    passage_rows = passages.shape[0]
    pieces = 4
    piece = passage_rows // pieces
    loads = []
    for h in range(heads):
        lanes = slice(h * HEAD_SIZE, (h + 1) * HEAD_SIZE)
        loads.append((key_ref.at[:, lanes], kv_weight.at[h, :, 0:HEAD_SIZE]))
        loads.append((value_ref.at[:, lanes], kv_weight.at[h, :, HEAD_SIZE : 2 * HEAD_SIZE]))
    kv_loads = len(loads)
    for i, ref in enumerate((query_ref, outer_ref, inner_ref, conv_ref)):
        loads.append((ref, in_weight.at[i]))
    loads.append((tokens_ref, tok.at[:, aligned(me, feat)]))
    token_loads = len(loads)
    for b, ref in enumerate((conv_out_ref, memory_out_ref)):
        for h in range(heads):
            loads.append(
                (
                    ref.at[h * HEAD_SIZE : (h + 1) * HEAD_SIZE, :],
                    out_weight.at[b * heads + h, aligned(me, HEAD_SIZE), :],
                )
            )
    loads = [pltpu.make_async_copy(s, d, load_sem.at[i]) for i, (s, d) in enumerate(loads)]
    store_loads = [
        pltpu.make_async_copy(
            store_ref.at[i * piece : (i + 1) * piece, :],
            passages.at[i * piece : (i + 1) * piece, :],
            store_sem.at[i],
        )
        for i in range(pieces)
    ]
    for copy in loads[:2] + store_loads + loads[token_loads:]:
        copy.start()

    barrier = pltpu.get_barrier_semaphore()
    for m in range(1, owners):
        pl.semaphore_signal(barrier, inc=1, device_id=(flip(st, m), me), device_id_type=MESH)
    for d in range(1, team):
        pl.semaphore_signal(
            barrier, inc=1, device_id=(st, lax.rem(me + d, team)), device_id_type=MESH
        )

    lane = lax.broadcasted_iota(jnp.int32, (owners, LANES), 1)
    row = lax.broadcasted_iota(jnp.int32, (owners, LANES), 0)
    requests = [(j, b) for j in range(NPB) for b in range(names_ref.shape[1])]
    filled = jnp.zeros((owners, LANES), jnp.int32)
    asks = jnp.zeros((owners, LANES), jnp.int32)
    over = jnp.zeros((owners, LANES), jnp.int32)
    for j, b in requests:
        hit = row == names_ref[j, b]
        asks = jnp.where(hit & (lane == filled), slots_ref[j, b], asks)
        if extra:
            late = jnp.where(hit & (filled >= direct) & (row // 4 != half), 1, 0)
            entry = (row % 4) * (2 * rest_slots) + filled - direct
            entry = jnp.sum(late * entry, axis=0, keepdims=True)
            late = jnp.sum(late, axis=0, keepdims=True)
            asks = jnp.where((late > 0) & (lane == capacity + over), entry, asks)
            over = over + late
        filled = jnp.where(hit, filled + 1, filled)
    asks = jnp.where(lane == LANES - 1, over, asks)
    for o in range(owners):
        asked[o, 0:1, :] = asks[o : o + 1, :]

    def project(h, i):
        found = jnp.dot(
            passages[i * piece : (i + 1) * piece, :],
            kv_weight[h],
            preferred_element_type=jnp.float32,
        ).astype(jnp.bfloat16)
        count = piece // PLEN
        for j in range(2):
            part = found[:, j * HEAD_SIZE : (j + 1) * HEAD_SIZE]
            table[2 * h + j][i * count : (i + 1) * count] = part.reshape(count, PLEN, HEAD_SIZE)

    def project_half(part):
        mine = range(part * pieces // 2, (part + 1) * pieces // 2)
        for i in mine:
            store_loads[i].wait()
        for i in mine:
            project(0, i)

    pl.semaphore_wait(barrier, owners - 1 + team - 1)

    def remote(src, dst, send, recv, device):
        return pltpu.make_async_remote_copy(
            src_ref=src,
            dst_ref=dst,
            send_sem=send,
            recv_sem=recv,
            device_id=device,
            device_id_type=MESH,
        )

    def ask(m, slot):
        return remote(
            asked.at[flip(st, m)],
            wanted.at[slot],
            ask_send.at[m],
            ask_recv.at[m],
            (flip(st, m), me),
        )

    for m in range(owners - 1, 0, -1):
        ask(m, st).start()
    loads[0].wait()
    loads[1].wait()
    project_half(0)

    def far_copy(k, c, owner):
        return remote(
            tokens_ref.at[aligned(c, SEQ_LEN), :],
            tok.at[aligned(c, SEQ_LEN), aligned(owner, feat)],
            far_send.at[k - 1, c],
            far_recv.at[k - 1, c],
            (st, up(k)),
        )

    def near_copy(c, owner):
        return remote(
            tokens_ref.at[aligned(c, SEQ_LEN), :],
            tok.at[aligned(c, SEQ_LEN), aligned(owner, feat)],
            near_send.at[c],
            near_recv.at[c],
            (st, partner),
        )

    def pass_copy(k, c, owner):
        place = tok.at[aligned(c, SEQ_LEN), aligned(owner, feat)]
        return remote(
            place, place, pass_send.at[k - 1, c], pass_recv.at[k - 1, c], (st, partner)
        )

    def w_near(owner):
        place = out_weight.at[:, aligned(owner, HEAD_SIZE), :]
        return remote(place, place, w_near_send, w_near_recv, (st, partner))

    def w_place(which, owner):
        return out_weight.at[which, aligned(owner, HEAD_SIZE), :]

    def w_far(k, owner):
        place = w_place(mine_piece, owner)
        return remote(place, place, w_far_send.at[k - 1], w_far_recv.at[k - 1], (st, up(k)))

    def w_side(m, k, which):
        place = w_place(which, down(k))
        return remote(
            place,
            place,
            w_side_send.at[m, k - 1],
            w_side_recv.at[m, k - 1],
            (flip(st, 1 if m == 3 else m), me),
        )

    def w_piece(m):
        return lax.rem(flip(st, m), parts) if m else mine_piece

    def w_sent(m):
        return w_piece(2) if m == 3 else mine_piece

    def w_turn():
        for k in range(1, chips):
            w_side(2, k, w_piece(2)).wait_recv()
            w_side(3, k, w_sent(3)).start()
            w_pass(2, k, down(k)).start()

    def w_pass(m, k, owner):
        place = w_place(w_piece(m), owner)
        return remote(
            place, place, w_pass_send.at[m, k - 1], w_pass_recv.at[m, k - 1], (st, partner)
        )

    for copy in loads[token_loads:]:
        copy.wait()
    for k in range(1, chips):
        w_far(k, me).start()
    w_near(me).start()

    @pl.loop(0, chunks)
    def _(c):
        for k in range(1, chips):
            far_copy(k, c, me).start()
        near_copy(c, me).start()

    def serve(i, m, slot):
        count = direct if m >= 4 else capacity
        return remote(
            staged[i].at[flip(st, m), 0:count],
            served[i].at[pl.ds(slot * capacity, count)],
            serve_send.at[i, m],
            serve_recv.at[i, m],
            (flip(st, m), me),
        )

    def beside_middle(j):
        return j + 2 * beside + 4 * half

    def spill(i, j):
        return remote(
            spill_out[i].at[j],
            spill_in[i].at[pl.ds((st % 4) * 2 * rest_slots, 2 * rest_slots)],
            spill_send.at[i, j],
            spill_recv.at[i, st % 4],
            (beside_middle(j), me),
        )

    def spill_arrival(i, source):
        return remote(
            spill_out[i].at[0],
            spill_in[i].at[pl.ds(source * 2 * rest_slots, 2 * rest_slots)],
            spill_send.at[i, 0],
            spill_recv.at[i, source],
            (source + 4 * half, me),
        )

    def far_reader(j, t):
        return j + 2 * t + 4 * beside

    def start_spill(i):
        for j in range(2):
            here = beside_middle(j) == st
            for t in range(2):
                for c in range(rest_slots):
                    found = table[i][wanted[far_reader(j, t), 0, direct + c]]
                    spill_out[i][j, t * rest_slots + c] = found

            @pl.when(here)
            def _():
                for n in range(2 * rest_slots):
                    spill_in[i][(st % 4) * 2 * rest_slots + n] = spill_out[i][j, n]

            @pl.when(jnp.logical_not(here))
            def _():
                spill(i, j).start()

    def packed_copy(i, t):
        return remote(
            packed[i].at[t],
            served[i].at[pl.ds(owners * capacity, extra)],
            packed_send.at[i, t],
            packed_recv.at[i],
            (far_reader(st % 2, t), me),
        )

    is_beside = (st // 2) % 2 == beside

    def relay(i):
        @pl.when(is_beside)
        def _():
            for source in range(4):

                @pl.when(source != st % 4)
                def _():
                    spill_arrival(i, source).wait_recv()

            for t in range(2):
                for n in range(extra):
                    entry = wanted[far_reader(st % 2, t), 0, capacity + n]
                    packed[i][t, n] = spill_in[i][entry + t * rest_slots]
            for t in range(2):
                packed_copy(i, t).start()

    def wait_served(i):
        for m in range(1, owners):
            serve(i, m, flip(st, m)).wait_recv()
        if extra:
            packed_copy(i, 0).wait_recv()

    def pass_weights():
        for k in range(1, chips):
            w_far(k, down(k)).wait_recv()
            for m in range(1, min(parts, 3)):
                w_side(m, k, mine_piece).start()
            w_pass(0, k, down(k)).start()

    project_half(1)
    for copy in loads[2:token_loads]:
        copy.start()
    own_asks = pltpu.make_async_copy(asked.at[st], wanted.at[st], smem_sem)
    own_asks.start()
    for m in range(1, owners):
        ask(m, flip(st, m)).wait_recv()
    own_asks.wait()
    for h in range(heads):
        if h:
            loads[2 * h].wait()
            loads[2 * h + 1].wait()
            for i in range(pieces):
                project(h, i)
        if extra:
            for i in (2 * h, 2 * h + 1):
                start_spill(i)
            if h == 1:
                relay(0)
                relay(1)
        if h == 1:
            pass_weights()
        for i in (2 * h, 2 * h + 1):
            for m in range(owners - 1, 0, -1):
                reader = flip(st, m)
                for c in range(direct if m >= 4 else capacity):
                    staged[i][reader, c] = table[i][wanted[reader, 0, c]]
                if m < owners - 1:
                    serve(i, m + 1, st).start()
            for c in range(capacity):
                served[i][st * capacity + c] = table[i][wanted[st, 0, c]]
            serve(i, 1, st).start()
    if heads == 1:
        pass_weights()

    late = jnp.int32(0)
    for f, (j, b) in enumerate(requests):
        name = names_ref[j, b]
        place = jnp.int32(0)
        for i, a in requests[:f]:
            place = place + jnp.where(names_ref[i, a] == name, 1, 0)
        where = name * capacity + place
        if extra:
            is_late = jnp.logical_and(place >= direct, name // 4 != half)
            where = jnp.where(is_late, owners * capacity + jnp.minimum(late, extra - 1), where)
            late = late + jnp.where(is_late, 1, 0)
        target[b * NPB + j] = where
    most = late
    for m in range(1, owners):
        most = jnp.maximum(most, wanted[flip(st, m), 0, LANES - 1])
    spilled_ref[0] = most

    for copy in loads[kv_loads:token_loads]:
        copy.wait()

    turn = chunks - 2
    row_number = lax.broadcasted_iota(jnp.int32, (SEQ_LEN, 1), 0)
    taps = taps_ref[...].astype(jnp.float32)

    @pl.loop(0, chunks)
    def _(c):
        if parts == 4:
            pl.when(c == turn)(w_turn)
        for k in range(1, chips):
            far_copy(k, c, down(k)).wait_recv()
            pass_copy(k, c, down(k)).start()
        near_copy(c, partner).wait_recv()
        for k in range(1, chips):
            pass_copy(k, c, down_other(k)).wait_recv()
        here = aligned(c, SEQ_LEN)
        x = tok[here, :]
        dot = functools.partial(jnp.dot, preferred_element_type=jnp.float32)
        queries[here, :] = dot(x, in_weight[0]).astype(jnp.bfloat16)
        mixed = dot(x, in_weight[2]) * dot(x, in_weight[3])
        filtered = jnp.zeros_like(mixed)
        for offset in range(CONV_K):
            back = CONV_K - 1 - offset
            shifted = mixed
            if back:
                shifted = jnp.where(row_number >= back, pltpu.roll(mixed, back, 0), 0.0)
            filtered = filtered + taps[offset : offset + 1, :] * shifted
        conv = (dot(x, in_weight[1]) * filtered).astype(jnp.bfloat16)
        for h in range(heads):
            branch[h][here, :] = conv[:, h * HEAD_SIZE : (h + 1) * HEAD_SIZE]

    if extra:
        for i in range(2 if heads > 1 else 0, parts):
            relay(i)

    others = [place(k) for k in range(1, chips) for place in (down, down_other)] + [partner]

    def row_send_copy(i, owner):
        d = lax.rem(owner - me + team, team)
        return remote(
            branch[i].at[aligned(owner, own_rows), :],
            moved[i].at[:, aligned(me, HEAD_SIZE)],
            row_send.at[i, d],
            row_recv.at[i, d],
            (st, owner),
        )

    def row_recv_copy(i, source):
        d = lax.rem(me - source + team, team)
        return remote(
            branch[i].at[aligned(source, own_rows), :],
            moved[i].at[:, aligned(source, HEAD_SIZE)],
            row_send.at[i, d],
            row_recv.at[i, d],
            (st, source),
        )

    def keep_rows(i):
        moved[i][:, aligned(me, HEAD_SIZE)] = branch[i][aligned(me, own_rows), :]

    def wait_rows(i):
        for source in others:
            row_recv_copy(i, source).wait_recv()

    for i in range(heads):
        for owner in others:
            row_send_copy(i, owner).start()
        keep_rows(i)

    gates[...] = jax.nn.sigmoid(
        lax.dot_general(
            tok[aligned(me, own_rows), :],
            gate_ref[...],
            (((1,), (1,)), ((), ())),
            preferred_element_type=jnp.float32,
        )
    )

    blocks = own_rows // BLOCK
    tile = 512
    tiles = out_weight.shape[2] // tile

    ones = jnp.ones((NPB * PLEN, HEAD_SIZE), jnp.bfloat16)

    def attention(h):
        def owner_powers(owner):
            for b in range(blocks):
                n = owner * blocks + b
                keys = jnp.concatenate(
                    [served[2 * h][target[n * NPB + j]] for j in range(NPB)], axis=0
                )
                scores = lax.dot_general(
                    queries[aligned(n, BLOCK), h * HEAD_SIZE : (h + 1) * HEAD_SIZE],
                    keys,
                    (((1,), (1,)), ((), ())),
                    preferred_element_type=jnp.float32,
                )
                scores = scores - jnp.max(scores, axis=1, keepdims=True)
                powers[aligned(n, BLOCK), :] = jnp.exp2(
                    scores * (HEAD_SIZE**-0.5 * LOG2_E)
                ).astype(jnp.bfloat16)

        def owner_rows(owner):
            numbers = [owner * blocks + b for b in range(blocks)]
            values = [
                jnp.concatenate(
                    [served[2 * h + 1][target[n * NPB + j]] for j in range(NPB)], axis=0
                )
                for n in numbers
            ]
            sums = [
                jnp.dot(
                    powers[aligned(n, BLOCK), :],
                    jnp.concatenate([value, ones], axis=1),
                    preferred_element_type=jnp.float32,
                )
                for n, value in zip(numbers, values)
            ]
            for n, both in zip(numbers, sums):
                branch[heads + h][aligned(n, BLOCK), :] = (
                    both[:, :HEAD_SIZE] / both[:, HEAD_SIZE:]
                ).astype(jnp.bfloat16)

        wait_served(2 * h)

        @pl.loop(0, team)
        def _(owner):
            owner_powers(owner)

        wait_served(2 * h + 1)
        for owner in others:
            owner_rows(owner)
            row_send_copy(heads + h, owner).start()
        owner_rows(me)
        keep_rows(heads + h)

    def add_memory(h, near, far, last):
        def add_tile(n):
            lanes = aligned(n, tile)
            value = total[:, lanes]
            for k in range(0 if near else 1, chips if far else 1):
                rows_of = aligned(lax.rem(chip + k, chips), CORES * HEAD_SIZE)
                value = value + gates[:, 1:2] * jnp.dot(
                    moved[heads + h][:, rows_of],
                    out_weight[heads + h, rows_of, lanes],
                    preferred_element_type=jnp.float32,
                )
            if last:
                out_ref[:, lanes] = value.astype(jnp.bfloat16)
            else:
                total[:, lanes] = value

        if last:
            for n in range(tiles):
                add_tile(n)
        else:
            pl.loop(0, tiles)(add_tile)

    for k in range(1, chips):
        for m in range(1, parts):
            if m != 2:
                w_side(m, k, w_piece(m)).wait_recv()
                w_pass(m, k, down(k)).start()

    def drain():
        for i in range(parts if extra else 0):
            for j in range(2):

                @pl.when(beside_middle(j) != st)
                def _():
                    spill(i, j).wait_send()

            @pl.when(is_beside)
            def _():
                for t in range(2):
                    packed_copy(i, t).wait_send()

        for m in range(1, owners):
            ask(m, st).wait_send()
            for i in range(2 * heads):
                serve(i, m, st).wait_send()

        @pl.loop(0, chunks)
        def _(c):
            for k in range(1, chips):
                far_copy(k, c, me).wait_send()
                pass_copy(k, c, down(k)).wait_send()
            near_copy(c, me).wait_send()

        for k in range(1, chips):
            w_far(k, me).wait_send()
            for m in range(parts):
                if m:
                    w_side(m, k, w_sent(m)).wait_send()
                w_pass(m, k, down(k)).wait_send()
        w_near(me).wait_send()

    for h in range(heads):
        attention(h)
        if h == 0:
            w_near(partner).wait_recv()
            for k in range(1, chips):
                for m in range(parts):
                    w_pass(m, k, down_other(k)).wait_recv()
            for i in range(heads):
                wait_rows(i)

            @pl.loop(0, tiles)
            def _(n):
                lanes = aligned(n, tile)
                value = 0.0
                for i in range(heads):
                    value = value + jnp.dot(
                        moved[i][...],
                        out_weight[i, :, lanes],
                        preferred_element_type=jnp.float32,
                    )
                total[:, lanes] = gates[:, 0:1] * value

        if h < heads - 1:
            wait_rows(heads + h)
            add_memory(h, True, True, False)
        else:
            row_recv_copy(heads + h, partner).wait_recv()
            add_memory(h, True, False, False)
            drain()
            for source in others[:-1]:
                row_recv_copy(heads + h, source).wait_recv()
            add_memory(h, False, True, True)

    for i in range(2 * heads):
        for owner in others:
            row_send_copy(i, owner).wait_send()


def fused(
    spills,
    tokens,
    store,
    passage_holder_index,
    passage_slot,
    query_weight,
    key_matrix,
    value_weight,
    outer_gate,
    inner_gate,
    conv_input,
    conv_taps,
    route_gate_projection,
    conv_out,
    memory_out,
):
    rows, feat = tokens.shape
    head_width = query_weight.shape[1]
    heads = head_width // HEAD_SIZE
    width = conv_out.shape[1]
    team = lax.axis_size("tp")
    owners = lax.axis_size("st")
    own_rows = rows // team
    depth = team * HEAD_SIZE
    chips = team // CORES
    chunks = rows // SEQ_LEN

    count = passage_holder_index.size
    capacity = max(2, 2 * count // owners)
    direct, extra = capacity, 0
    if spills:
        direct = (5 * capacity + 7) // 8
        extra = count * 3 // 16
    flat_rows = store.reshape(-1, store.shape[-1])
    held = store.shape[0]
    bf16, f32 = jnp.bfloat16, jnp.float32
    dma = pltpu.SemaphoreType.DMA
    scratch = [
        pltpu.VMEM((rows, team * feat), bf16),
        pltpu.VMEM(flat_rows.shape, bf16),
        pltpu.VMEM((4, team * feat, head_width), bf16),
        pltpu.VMEM((heads, team * feat, 2 * HEAD_SIZE), bf16),
        pltpu.VMEM((2 * heads, depth, width), bf16),
        pltpu.VMEM((own_rows, width), f32),
        pltpu.VMEM((rows, head_width), bf16),
        pltpu.VMEM((own_rows, 2), f32),
        pltpu.VMEM((rows, NPB * PLEN), bf16),
        pltpu.VMEM((owners, 8, LANES), jnp.int32),
        pltpu.SMEM((owners, 8, LANES), jnp.int32),
        pltpu.SMEM((count,), jnp.int32),
    ]
    scratch += [pltpu.VMEM((held, PLEN, HEAD_SIZE), bf16)] * (2 * heads)
    scratch += [pltpu.VMEM((owners, capacity, PLEN, HEAD_SIZE), bf16)] * (2 * heads)
    scratch += [pltpu.VMEM((owners * capacity + extra, PLEN, HEAD_SIZE), bf16)] * (2 * heads)
    if spills:
        rest_slots = capacity - direct
        scratch += [pltpu.VMEM((2, 2 * rest_slots, PLEN, HEAD_SIZE), bf16)] * (2 * heads)
        scratch += [pltpu.VMEM((8 * rest_slots, PLEN, HEAD_SIZE), bf16)] * (2 * heads)
        scratch += [pltpu.VMEM((2, extra, PLEN, HEAD_SIZE), bf16)] * (2 * heads)
    scratch += [pltpu.VMEM((rows, HEAD_SIZE), bf16)] * (2 * heads)
    scratch += [pltpu.VMEM((own_rows, depth), bf16)] * (2 * heads)
    scratch += [
        dma((4 * heads + 5,)),
        dma((4,)),
        dma,
        dma((owners,)),
        dma((owners,)),
        dma((chunks,)),
        dma((chunks,)),
        dma((chips - 1, chunks)),
        dma((chips - 1, chunks)),
        dma((chips - 1, chunks)),
        dma((chips - 1, chunks)),
        dma((2 * heads, owners)),
        dma((2 * heads, owners)),
        dma((2 * heads, team)),
        dma((2 * heads, team)),
        dma,
        dma,
        dma((chips - 1,)),
        dma((chips - 1,)),
        dma((2 * heads, chips - 1)),
        dma((2 * heads, chips - 1)),
        dma((2 * heads, chips - 1)),
        dma((2 * heads, chips - 1)),
        dma((2 * heads, 2)),
        dma((2 * heads, 4)),
        dma((2 * heads, 2)),
        dma((2 * heads,)),
    ]
    smem = pl.BlockSpec(memory_space=pltpu.SMEM)
    vmem = pl.BlockSpec(memory_space=pltpu.VMEM)
    hbm = pl.BlockSpec(memory_space=pltpu.HBM)
    return pl.pallas_call(
        functools.partial(fused_kernel, (owners, team, heads, capacity, direct, extra, rows, feat)),
        out_shape=(
            pltpu.VMEM((own_rows, width), bf16),
            pltpu.SMEM((1,), jnp.int32),
        ),
        in_specs=[smem, smem] + [hbm] * 8 + [vmem, vmem] + [hbm] * 2,
        out_specs=(vmem, smem),
        scratch_shapes=scratch,
        compiler_params=pltpu.CompilerParams(
            collective_id=int(spills), has_side_effects=True, vmem_limit_bytes=61 * 1024 * 1024
        ),
    )(
        passage_holder_index.T,
        passage_slot.T,
        tokens,
        flat_rows,
        key_matrix,
        value_weight,
        query_weight,
        outer_gate,
        inner_gate,
        conv_input,
        conv_taps,
        route_gate_projection.T,
        conv_out,
        memory_out,
    )


def local(*args):
    count, owners = args[2].size, lax.axis_size("st")
    if owners != 8:
        return fused(False, *args)[0]
    result, most = fused(True, *args)
    return lax.cond(
        most[0] > count * 3 // 16, lambda: fused(False, *args)[0], lambda: result
    )


def solution(mesh):
    return jax.shard_map(
        local,
        mesh=mesh,
        in_specs=(
            P("st", "tp"),
            P("st", None, None),
            P("st", None),
            P("st", None),
            P(None, "tp"),
            P(None, "tp"),
            P(None, "tp"),
            P(None, "tp"),
            P(None, "tp"),
            P(None, "tp"),
            P(None, "tp"),
            P(),
            P("tp", None),
            P("tp", None),
        ),
        out_specs=P(("st", "tp"), None),
        check_vma=False,
    )
```
